32 devices in a mesh: sp: 8 (over z, y), tp: 4 (over x, core).
Axes of the slice: x: 2, y: 2, z: 4, core: 2. Of those that a mesh axis runs over, the one named last changes fastest.
Arguments:
- activations: bfloat16 [6144, 2048], P(('sp', 'tp')), may hold values from -6 to 6
- in_gain: float32 [2048], replicated, may hold values from 0.1 to 1.9
- w_pool_in: bfloat16 [2048, 1024], P(None, 'tp'), may hold values from -0.125 to 0.125
- pool_gain: float32 [1024], P('tp'), may hold values from 0.1 to 1.9
- w_qlat: bfloat16 [2048, 768], P(None, 'tp'), may hold values from -0.125 to 0.125
- w_kvlat: bfloat16 [2048, 512], P(None, 'tp'), may hold values from -0.125 to 0.125
- w_krope: bfloat16 [2048, 32], replicated, may hold values from -0.125 to 0.125
- qlat_gain: float32 [768], replicated, may hold values from 0.1 to 1.9
- kvlat_gain: float32 [512], replicated, may hold values from 0.1 to 1.9
- w_qup: bfloat16 [768, 1536], P(None, 'tp'), may hold values from -0.21875 to 0.21875
- w_kup: bfloat16 [512, 1024], P(None, 'tp'), may hold values from -0.25 to 0.25
- w_vup: bfloat16 [512, 1024], P(None, 'tp'), may hold values from -0.25 to 0.25
- qhead_gain: float32 [96], replicated, may hold values from 1.1 to 1.9
- khead_gain: float32 [96], replicated, may hold values from 1.1 to 1.9
- w_out_pool: bfloat16 [1024, 2048], P('tp'), may hold values from -0.1875 to 0.1875
- w_out_attn: bfloat16 [1024, 2048], P('tp'), may hold values from -0.75 to 0.75
Outputs:
- mixed: bfloat16 [6144, 2048], P(('sp', 'tp'))
The draws below stay inside these ranges and needn't reach their ends.
All inputs are finite; a program needn't handle non-finite values.
Results may differ from the reference program's by a relative error of at most 0.025.
Values may be sent and summed in bfloat16 or wider, within the bound.
A program may use at most 128 MiB of HBM per device.

```python
import math
import jax
import jax.numpy as jnp
from jax import lax

D = 2048
POOL = 1024
GROUP = 256
HEADS = 16
NOPE = 64
ROPE = 32
VDIM = 64
QLAT = 768
KVLAT = 512
TOKENS = 6144
N_TP = 4


def level_of(stream_key, extent, split, low, top_value):
    def one(axis_at, shards_of):
        draws = jax.random.uniform(jax.random.fold_in(jax.random.fold_in(stream_key, 6), axis_at), (shards_of,), jnp.float32, low / len(split), top_value / len(split))
        return jnp.repeat(jnp.exp(draws), extent[axis_at] // shards_of).reshape((-1,) + (1,) * (len(extent) - axis_at - 1))

    level = one(*split[0])
    for cut in split[1:]:
        level = level * one(*cut)
    return level


def noise(own_key, shape, scale, reach, cuts=(), kind=jnp.bfloat16):
    array = jax.random.normal(own_key, shape, jnp.float32) * scale
    if len(cuts) > 0:
        array = level_of(own_key, shape, cuts, -0.22, 0.18) * array
    return jnp.clip(array, min=-reach, max=reach).astype(kind)


def setup_inputs(seed: int = 0) -> dict:
    streams_of = jax.random.split(jax.random.key(seed), 17)
    activations = noise(streams_of[0], (TOKENS, D), 1.0, 6.0, ((0, 32),))
    in_gain = jnp.clip(1.0 + 0.18 * jax.random.normal(streams_of[1], (D,), jnp.float32), 0.1, 1.9)
    w_pool_in = noise(streams_of[2], (D, POOL), D ** -0.5, 0.125, ((1, 4),))
    pool_gain = jnp.clip(1.0 + 0.18 * jax.random.normal(streams_of[3], (POOL,), jnp.float32), 0.1, 1.9)
    w_qlat = noise(streams_of[4], (D, QLAT), D ** -0.5, 0.125, ((1, 4),))
    w_kvlat = noise(streams_of[5], (D, KVLAT), D ** -0.5, 0.125, ((1, 4),))
    w_krope = noise(streams_of[6], (D, ROPE), D ** -0.5, 0.125)
    qlat_gain = jnp.clip(1.0 + 0.18 * jax.random.normal(streams_of[7], (QLAT,), jnp.float32), 0.1, 1.9)
    kvlat_gain = jnp.clip(1.0 + 0.18 * jax.random.normal(streams_of[8], (KVLAT,), jnp.float32), 0.1, 1.9)
    w_qup = noise(streams_of[9], (QLAT, HEADS * (NOPE + ROPE)), QLAT ** -0.5, 0.21875, ((1, 4),))
    w_kup = noise(streams_of[10], (KVLAT, HEADS * NOPE), KVLAT ** -0.5, 0.25, ((1, 4),))
    w_vup = noise(streams_of[11], (KVLAT, HEADS * VDIM), KVLAT ** -0.5, 0.25, ((1, 4),))
    qhead_gain = jnp.clip(jax.random.uniform(streams_of[12], (NOPE + ROPE,), jnp.float32, 1.1, 1.9), 1.1, 1.9)
    khead_gain = jnp.clip(jax.random.uniform(streams_of[13], (NOPE + ROPE,), jnp.float32, 1.1, 1.9), 1.1, 1.9)
    w_out_pool = noise(streams_of[14], (POOL, D), POOL ** -0.5, 0.1875, ((0, 4),))
    w_out_attn = noise(streams_of[15], (HEADS * VDIM, D), (HEADS * VDIM // 16) ** -0.5, 0.75, ((0, 4),))
    return {"activations": activations, "in_gain": in_gain, "w_pool_in": w_pool_in, "pool_gain": pool_gain, "w_qlat": w_qlat, "w_kvlat": w_kvlat, "w_krope": w_krope, "qlat_gain": qlat_gain, "kvlat_gain": kvlat_gain, "w_qup": w_qup, "w_kup": w_kup, "w_vup": w_vup, "qhead_gain": qhead_gain, "khead_gain": khead_gain, "w_out_pool": w_out_pool, "w_out_attn": w_out_attn}


norm_eps = 1e-06
rope_theta = 10000.0
rim_depth = 15
block_rows = 512

def row_norm(source, norm_gain):
    as_float = source.astype(jnp.float32)
    factor = lax.rsqrt(lax.optimization_barrier(jnp.mean(as_float * as_float, axis=-1, keepdims=True)) + norm_eps)
    return as_float * factor * norm_gain

def rotate(head_rows, positions):
    half_rope = ROPE // 2
    frequency = rope_theta ** (-jnp.arange(0, ROPE, 2, dtype=jnp.float32) / ROPE)
    angles = positions.astype(jnp.float32)[:, None] * frequency[None, :]
    cosine = jnp.cos(angles)[:, None, :]
    sine_part = jnp.sin(angles)[:, None, :]
    plain_part = head_rows[..., :NOPE]
    lower_half = head_rows[..., NOPE:NOPE + half_rope]
    upper_half = head_rows[..., NOPE + half_rope:]
    return jnp.concatenate([plain_part, lower_half * cosine - upper_half * sine_part, upper_half * cosine + lower_half * sine_part], axis=-1)

def pool_mix(extended, positions, channel_start):
    row_count = positions.shape[0]
    width = extended.shape[1]
    channel = channel_start + jnp.arange(width, dtype=jnp.int32)
    window = jnp.left_shift(jnp.int32(2), (channel // GROUP).astype(jnp.int32))
    as_float = extended.astype(jnp.float32)
    window_sum = jnp.zeros((row_count, width), jnp.float32)
    for lag_index in range(rim_depth + 1):
        lagged = as_float[rim_depth - lag_index:rim_depth - lag_index + row_count]
        window_sum = window_sum + jnp.where(lag_index < window[None, :], lagged, 0.0)
    divisor = jnp.minimum(positions[:, None] + 1, window[None, :]).astype(jnp.float32)
    return window_sum / divisor - as_float[rim_depth:]

def make_queries(q_normed, w_qup, norm_gain, positions):
    row_count = q_normed.shape[0]
    head_count = w_qup.shape[1] // (NOPE + ROPE)
    query_raw = jnp.dot(q_normed, w_qup, preferred_element_type=jnp.float32).astype(jnp.bfloat16)
    query_raw = query_raw.reshape(row_count, head_count, NOPE + ROPE)
    return rotate(row_norm(query_raw, norm_gain), positions).astype(jnp.bfloat16)

def make_keys(kv_rows, rope_rows, w_kup, w_vup, norm_gain, positions):
    row_count = kv_rows.shape[0]
    head_count = w_kup.shape[1] // NOPE
    key_plain = jnp.dot(kv_rows, w_kup, preferred_element_type=jnp.float32).astype(jnp.bfloat16)
    key_plain = key_plain.reshape(row_count, head_count, NOPE)
    value_rows = jnp.dot(kv_rows, w_vup, preferred_element_type=jnp.float32).astype(jnp.bfloat16)
    shared = jnp.broadcast_to(rope_rows[:, None, :], (row_count, head_count, ROPE))
    joined = jnp.concatenate([key_plain, shared], axis=-1)
    key_rows = rotate(row_norm(joined, norm_gain), positions).astype(jnp.bfloat16)
    return (key_rows.reshape(row_count, head_count * (NOPE + ROPE)), value_rows)

def attend(queries, key_rows, value_rows):
    all_rows, head_count, _ = queries.shape
    block_size = math.gcd(block_rows, all_rows)
    key_rows = key_rows.reshape(all_rows, head_count, NOPE + ROPE)
    value_rows = value_rows.reshape(all_rows, head_count, VDIM)
    score_scale = (NOPE + ROPE) ** (-0.5)

    def one_block(block_index):
        first_row = block_index * block_size
        query_block = lax.dynamic_slice_in_dim(queries, first_row, block_size, 0).astype(jnp.float32)
        query_pos = first_row + jnp.arange(block_size, dtype=jnp.int32)

        def add_keys(key_index, state_pair):
            numerator, denominator = state_pair
            key_first = key_index * block_size
            key_block = lax.dynamic_slice_in_dim(key_rows, key_first, block_size, 0).astype(jnp.float32)
            value_block = lax.dynamic_slice_in_dim(value_rows, key_first, block_size, 0).astype(jnp.float32)
            key_pos = key_first + jnp.arange(block_size, dtype=jnp.int32)
            scores = jnp.einsum('qhd,khd->hqk', query_block, key_block) * score_scale
            weights = jnp.where(key_pos[None, None, :] <= query_pos[None, :, None], jnp.exp(scores), 0.0)
            denominator = denominator + lax.optimization_barrier(jnp.sum(weights, axis=-1))
            rounded = lax.optimization_barrier(weights.astype(jnp.bfloat16)).astype(jnp.float32)
            numerator = numerator + jnp.einsum('hqk,khd->qhd', rounded, value_block)
            return (numerator, denominator)
        start_pair = (jnp.zeros((block_size, head_count, VDIM), jnp.float32), jnp.zeros((head_count, block_size), jnp.float32))
        numerator, denominator = lax.fori_loop(0, block_index + 1, add_keys, start_pair)
        return (numerator / jnp.transpose(denominator)[:, :, None]).astype(jnp.bfloat16)
    blocks_out = lax.map(one_block, jnp.arange(all_rows // block_size, dtype=jnp.int32))
    return blocks_out.reshape(all_rows, head_count * VDIM)

def reference(activations, in_gain, w_pool_in, pool_gain, w_qlat, w_kvlat, w_krope, qlat_gain, kvlat_gain, w_qup, w_kup, w_vup, qhead_gain, khead_gain, w_out_pool, w_out_attn):
    positions = jnp.arange(TOKENS, dtype=jnp.int32)
    normed = row_norm(activations, in_gain).astype(jnp.bfloat16)
    pool_in = jnp.dot(normed, w_pool_in, preferred_element_type=jnp.float32).astype(jnp.bfloat16)
    extended = jnp.concatenate([jnp.zeros((rim_depth, POOL), jnp.bfloat16), pool_in], axis=0)
    pool_out = (pool_mix(extended, positions, 0) * pool_gain).astype(jnp.bfloat16)
    q_latent = jnp.dot(normed, w_qlat, preferred_element_type=jnp.float32).astype(jnp.bfloat16)
    kv_latent = jnp.dot(normed, w_kvlat, preferred_element_type=jnp.float32).astype(jnp.bfloat16)
    rope_key = jnp.dot(normed, w_krope, preferred_element_type=jnp.float32).astype(jnp.bfloat16)
    q_normed = row_norm(q_latent, qlat_gain).astype(jnp.bfloat16)
    kv_normed = row_norm(kv_latent, kvlat_gain).astype(jnp.bfloat16)
    queries = make_queries(q_normed, w_qup, qhead_gain, positions)
    key_rows, value_rows = make_keys(kv_normed, rope_key, w_kup, w_vup, khead_gain, positions)
    attended = attend(queries, key_rows, value_rows)
    pool_span = POOL // N_TP
    attn_span = HEADS * VDIM // N_TP
    mixed = jnp.zeros((TOKENS, D), jnp.float32)
    for block_index in range(N_TP):
        pool_lo = block_index * pool_span
        attn_lo = block_index * attn_span
        partial_value = jnp.dot(pool_out[:, pool_lo:pool_lo + pool_span], w_out_pool[pool_lo:pool_lo + pool_span], preferred_element_type=jnp.float32)
        partial_value = partial_value + jnp.dot(attended[:, attn_lo:attn_lo + attn_span], w_out_attn[attn_lo:attn_lo + attn_span], preferred_element_type=jnp.float32)
        rounded = lax.optimization_barrier(partial_value.astype(jnp.bfloat16)).astype(jnp.float32)
        mixed = mixed + rounded
    return mixed.astype(jnp.bfloat16)
```

```python
import functools
import math

import jax
import jax.numpy as jnp
import numpy as np
from jax import lax
from jax.experimental import pallas as pl
from jax.experimental.pallas import tpu as pltpu
from jax.sharding import PartitionSpec as P

GROUP = 256
NOPE = 64
ROPE = 32
VDIM = 64
HEAD = NOPE + ROPE
HALF = ROPE // 2
LANES = 128
RIM = 16
CHUNKS = 3
COLS = 4

norm_eps = 1e-06
rope_theta = 10000.0
bf16 = jnp.bfloat16
f32 = jnp.float32
MESH = pl.DeviceIdType.MESH
NT = (((1,), (1,)), ((), ()))


def up_to(n, m):
    return (n + m - 1) // m * m


def dot(a, b):
    return jnp.dot(a, b, preferred_element_type=f32)


def dot_nt(a, b):
    return lax.dot_general(a, b, NT, preferred_element_type=f32)


def remote(src, dst, send_sem, recv_sem, target):
    return pltpu.make_async_remote_copy(
        src_ref=src, dst_ref=dst, send_sem=send_sem, recv_sem=recv_sem, device_id=target, device_id_type=MESH
    )


def padded_transpose(w):
    rows, cols = w.shape
    r, c = up_to(rows, LANES), up_to(cols, LANES)
    w = w.astype(f32)
    if r > rows:
        w = jnp.concatenate([w, jnp.zeros((r - rows, cols), f32)], axis=0)
    if c > cols:
        w = jnp.concatenate([w, jnp.zeros((r, c - cols), f32)], axis=1)
    return w.T[:cols]


def mixer_kernel(
    n_sp,
    n_tp,
    x_hbm,
    wpool_hbm,
    wq_hbm,
    wkv_hbm,
    wkr_hbm,
    wqup_hbm,
    wkup_hbm,
    wvup_hbm,
    wop_hbm,
    woa_hbm,
    in_gain,
    pool_gain,
    qlat_gain,
    kvlat_gain,
    qh_gain,
    kh_gain,
    cos_q,
    sin_q,
    cos_k,
    sin_k,
    cos_b,
    sin_b,
    out_ref,
    x_own,
    wpool,
    wq_raw,
    wkv_raw,
    wkr_raw,
    wqup,
    wkup,
    wvup,
    wo,
    wo_p,
    wq_cat,
    wkv_cat,
    wq_t,
    wk_t,
    wv_pad,
    xg,
    qx,
    kv_mine,
    kvx,
    rope_own,
    kv_all,
    pool_ext,
    queries,
    keys_t,
    values,
    acc,
    act,
    act_p,
    f_out,
    f_in,
    ld_sem,
    a_far_send,
    a_near_send,
    a_relay_send,
    a_recv,
    kv_send,
    kv_recv,
    q_far_send,
    q_near_send,
    q_relay_send,
    q_recv,
    up_send,
    side_send,
    near_send,
    d_recv,
    p_send,
    p_recv,
    wo_send,
    wo_recv,
    act_send,
    act_recv,
    f_send,
    f_recv,
):
    me = lax.axis_index("tp")
    core, chip = lax.rem(me, 2), lax.div(me, 2)
    chips = n_tp // 2
    partner = me + 1 - 2 * core
    shard = lax.axis_index("sp")
    deep, side = lax.div(shard, 2), lax.rem(shard, 2)
    last_deep = n_sp // 2 - 1
    other = shard + 1 - 2 * side

    r, width = x_own.shape
    rows = r * n_tp
    half = r * chips
    qc = wq_raw.shape[1]
    kc = wkv_raw.shape[1]
    kvlat = kc * n_tp
    pc = wpool.shape[1]
    heads = wkup.shape[1] // NOPE
    hc = heads * VDIM
    rc = r // CHUNKS

    loads = {}

    def load(i, name, src, dst):
        loads[name] = pltpu.make_async_copy(src, dst, ld_sem.at[i])
        loads[name].start()

    load(0, "x", x_hbm, x_own)
    load(1, "wkv", wkv_hbm, wkv_raw)
    load(2, "wkr", wkr_hbm, wkr_raw)
    load(3, "wq", wq_hbm, wq_raw)
    load(4, "wpool", wpool_hbm, wpool)
    load(5, "wqup", wqup_hbm, wqup)
    load(6, "wkup", wkup_hbm, wkup)
    load(7, "wvup", wvup_hbm, wvup)
    load(8, "wop", wop_hbm, wo.at[pl.ds(0, pc), :])
    load(9, "woa", woa_hbm, wo.at[pl.ds(pc, hc), :])

    barrier = pltpu.get_barrier_semaphore()
    for step in range(1, n_tp):
        pl.semaphore_signal(
            barrier, inc=1, device_id={"tp": lax.rem(me + step, n_tp)}, device_id_type=MESH
        )
    greeted = n_tp - 1
    for gap in (-2, -1, 1, 2):
        there = shard + gap
        valid = (there >= 0) & (there < n_sp)

        @pl.when(valid)
        def _():
            pl.semaphore_signal(barrier, inc=1, device_id={"sp": there}, device_id_type=MESH)

        greeted = greeted + jnp.where(valid, 1, 0)
    pl.semaphore_wait(barrier, greeted)

    def place(k, c):
        return 2 * k + c

    def behind(step):
        return lax.rem(chip + chips - step, chips)

    def ahead(step):
        return lax.rem(chip + step, chips)

    def rows_at(g, off, count):
        return pl.ds(pl.multiple_of(g * r + off, 16), count)

    def arrived(ref, sem):
        remote(ref, ref, a_near_send.at[0], sem, {"tp": partner}).wait_recv()

    sends = []
    loads["x"].wait()
    for c in range(CHUNKS):
        at = pl.ds(c * rc, rc)
        xf = x_own[at, :].astype(f32)
        factor = lax.rsqrt(jnp.mean(xf * xf, axis=1, keepdims=True) + norm_eps)
        xg[me, at, :] = (xf * factor * in_gain[...]).astype(bf16)
        own = xg.at[me, at, :]
        for step in range(1, chips):
            copy = remote(
                own, own, a_far_send.at[step - 1, c], a_recv.at[me, c], {"tp": place(ahead(step), core)}
            )
            copy.start()
            sends.append(copy)
    for c in range(CHUNKS):
        own = xg.at[me, pl.ds(c * rc, rc), :]
        copy = remote(own, own, a_near_send.at[c], a_recv.at[me, c], {"tp": partner})
        copy.start()
        sends.append(copy)

    loads["wkv"].wait()
    loads["wkr"].wait()
    wkv_cat[...] = jnp.zeros_like(wkv_cat)
    wkv_cat[:, :kc] = wkv_raw[...]
    wkv_cat[:, LANES : LANES + ROPE] = wkr_raw[...]
    loads["wq"].wait()
    wq_cat[...] = jnp.zeros_like(wq_cat)
    wq_cat[:, :qc] = wq_raw[...]
    loads["wpool"].wait()

    def project(k, c, off, count, same_core):
        g = place(k, c)
        xs = xg[g, pl.ds(off, count), :]
        at = rows_at(g, off, count)
        both = dot(xs, wkv_cat[...])
        kv_mine[c, k, pl.ds(off, count), :] = both[:, :kc].astype(bf16)
        if same_core:
            shared = both[:, LANES : 2 * LANES].astype(bf16).astype(f32)
            rope_own[pl.ds(pl.multiple_of(k * r + off, 8), count), :] = shared
        qx[me, at, :] = dot(xs, wq_cat[...]).astype(bf16)
        at_ext = pl.ds(pl.multiple_of(g * r + off + RIM, 16), count)
        pool_ext[at_ext, :] = dot(xs, wpool[...]).astype(bf16)

    project(chip, core, 0, r, True)
    for c in range(CHUNKS):
        arrived(xg.at[partner, pl.ds(c * rc, rc), :], a_recv.at[partner, c])
    project(chip, 1 - core, 0, r, False)

    loads["wqup"].wait()
    for src in range(n_tp):
        part = wqup[src * qc : (src + 1) * qc, :].astype(f32) * qlat_gain[src * qc : (src + 1) * qc, :]
        wq_t[src] = padded_transpose(part).astype(bf16)
    loads["wkup"].wait()
    wk_t[...] = padded_transpose(wkup[...]).astype(bf16)
    loads["wvup"].wait()
    wv_pad[...] = jnp.zeros_like(wv_pad)
    for h in range(heads):
        wv_pad[:, h * LANES : h * LANES + VDIM] = (
            wvup[...].astype(f32)[:, h * VDIM : (h + 1) * VDIM].astype(bf16)
        )
    keys_t[:, HEAD:, :] = jnp.zeros((heads, LANES - HEAD, rows), bf16)
    acc[...] = jnp.zeros_like(acc)

    loads["wop"].wait()
    loads["woa"].wait()
    wo_copy = remote(wo, wo_p, wo_send, wo_recv, {"tp": partner})
    wo_copy.start()

    for c in range(CHUNKS):
        at = pl.ds(c * rc, rc)
        for step in range(1, chips):
            g = place(behind(step), core)
            block = xg.at[g, at, :]
            arrived(block, a_recv.at[g, c])
            copy = remote(block, block, a_relay_send.at[step - 1, c], a_recv.at[g, c], {"tp": partner})
            copy.start()
            sends.append(copy)
        for step in range(1, chips):
            project(behind(step), core, c * rc, rc, True)
        for step in range(1, chips):
            g = place(behind(step), 1 - core)
            arrived(xg.at[g, at, :], a_recv.at[g, c])
            project(behind(step), 1 - core, c * rc, rc, False)

    for step in range(1, n_tp):
        there = lax.rem(me + step, n_tp)
        copy = remote(
            kv_mine.at[lax.rem(there, 2)], kvx.at[me], kv_send.at[step - 1], kv_recv.at[me], {"tp": there}
        )
        copy.start()
        sends.append(copy)
    own_q = qx.at[me]
    for step in range(1, chips):
        copy = remote(own_q, own_q, q_far_send.at[step - 1], q_recv.at[me], {"tp": place(ahead(step), core)})
        copy.start()
        sends.append(copy)
    copy = remote(own_q, own_q, q_near_send, q_recv.at[me], {"tp": partner})
    copy.start()
    sends.append(copy)

    rim_copy = remote(
        pool_ext.at[pl.ds(rows, RIM), :], pool_ext.at[pl.ds(0, RIM), :], p_send, p_recv, {"sp": shard + 1}
    )

    @pl.when(shard < n_sp - 1)
    def _():
        rim_copy.start()

    @pl.when(shard == 0)
    def _():
        pool_ext[pl.ds(0, RIM), :] = jnp.zeros((RIM, pc), bf16)

    kvx[me] = kv_mine[core]
    for step in range(1, n_tp):
        source = lax.rem(me + step, n_tp)
        arrived(kvx.at[source], kv_recv.at[source])
    lat = jnp.concatenate([kvx[i].reshape(half, kc).astype(f32) for i in range(n_tp)], axis=1)
    factor = lax.rsqrt(jnp.mean(lat * lat, axis=1, keepdims=True) + norm_eps)
    kv_all[shard, core, pl.ds(0, half), :] = (lat * factor * kvlat_gain[...]).astype(bf16)
    kv_all[shard, core, pl.ds(half, ROPE), pl.ds(0, half)] = rope_own[...].T[:ROPE].astype(bf16)

    def piece(block, h):
        return kv_all.at[block, h]

    def onward(block):
        return remote(
            piece(block, core), piece(block, core), up_send.at[block], d_recv.at[block, core], {"sp": shard + 2}
        )

    def across(block):
        return remote(
            piece(block, core), piece(block, core), side_send.at[block], d_recv.at[block, core], {"sp": other}
        )

    def near(block):
        return remote(
            piece(block, core), piece(block, core), near_send.at[block], d_recv.at[block, core], {"tp": partner}
        )

    @pl.when(deep < last_deep)
    def _():
        onward(shard).start()

    @pl.when(side == 0)
    def _():
        across(shard).start()

    near(shard).start()

    for step in range(1, chips):
        g = place(behind(step), core)
        arrived(qx.at[g], q_recv.at[g])
        copy = remote(qx.at[g], qx.at[g], q_relay_send.at[step - 1], q_recv.at[g], {"tp": partner})
        copy.start()
        sends.append(copy)
    for k in range(chips):
        g = place(k, 1 - core)
        arrived(qx.at[g], q_recv.at[g])

    score_scale = HEAD ** (-0.5) * math.log2(math.e)
    q_tile = 2 * r

    def table(cos_ref, sin_ref, block, at):
        ca, sa = cos_ref[:, at], sin_ref[:, at]
        cb, sb = cos_b[block], sin_b[block]
        return ca * cb - sa * sb, sa * cb + ca * sb

    def make_queries(i, _):
        at = pl.ds(pl.multiple_of(i * LANES, LANES), LANES)
        raw = None
        squares = None
        ones = jnp.ones((8, qx.shape[2]), bf16)
        for src in range(n_tp):
            part = qx[src, at, :]
            term = dot_nt(wq_t[src], part)
            raw = term if raw is None else raw + term
            pf = part.astype(f32)
            term = dot_nt(ones, (pf * pf).astype(bf16))
            squares = term if squares is None else squares + term
        eps = norm_eps * (squares[:1] * (1.0 / (qc * n_tp)) + norm_eps)
        cosine, sine = table(cos_q, sin_q, shard, at)
        for h in range(heads):
            x = raw[h * HEAD : (h + 1) * HEAD]
            factor = lax.rsqrt(jnp.sum(x * x, axis=0, keepdims=True) * (1.0 / HEAD) + eps) * score_scale
            y = x * factor * qh_gain[...]
            low, high = y[NOPE : NOPE + HALF], y[NOPE + HALF :]
            full = jnp.concatenate(
                [
                    y[:NOPE] * kh_gain[:NOPE, :],
                    low * cosine - high * sine,
                    high * cosine + low * sine,
                    jnp.zeros((LANES - HEAD, LANES), f32),
                ],
                axis=0,
            )
            queries[h, at, :] = full.T.astype(bf16)
        return 0

    lax.fori_loop(0, rows // LANES, make_queries, 0)

    lane = lax.broadcasted_iota(jnp.int32, (half, LANES), 1)

    def prepare(block):
        for c in range(2):
            at = pl.ds(c * half, half)
            lat = kv_all[block, c, pl.ds(0, half), :]
            shared = kv_all[block, c, pl.ds(half, ROPE), pl.ds(0, half)].astype(f32)
            shared_sq = jnp.sum(shared * shared, axis=0, keepdims=True)
            cosine, sine = table(cos_k, sin_k, block, at)
            gained = shared * kh_gain[NOPE:, :]
            low, high = gained[:HALF], gained[HALF:]
            turned = jnp.concatenate([low * cosine - high * sine, high * cosine + low * sine], axis=0)
            plain = dot_nt(wk_t[...], lat)
            value = dot(lat, wv_pad[...])
            for h in range(heads):
                x = plain[h * NOPE : (h + 1) * NOPE]
                total = jnp.sum(x * x, axis=0, keepdims=True) + shared_sq
                factor = lax.rsqrt(total * (1.0 / HEAD) + norm_eps)
                keys_t[h, :NOPE, at] = (x * factor).astype(bf16)
                keys_t[h, NOPE:HEAD, at] = (turned * factor).astype(bf16)
                v = jnp.where(lane == VDIM, 1.0, value[:, h * LANES : (h + 1) * LANES])
                values[h, at, :] = v.astype(bf16)

    key_tile = math.gcd(half, 384)

    def accumulate(i, masked):
        at = pl.ds(pl.multiple_of(i * q_tile, q_tile), q_tile)
        for h in range(heads):
            q = queries[h, at, :]
            total = acc[h, at, :]
            for j in range(rows // key_tile):
                cols = pl.ds(j * key_tile, key_tile)
                weights = jnp.exp2(dot(q, keys_t[h, :, cols]))
                if masked:
                    q_pos = i * q_tile + lax.broadcasted_iota(jnp.int32, weights.shape, 0)
                    col = (j * key_tile) % half + lax.broadcasted_iota(jnp.int32, weights.shape, 1)
                    k_pos = col + ((j * key_tile) // half) * r
                    for k in range(1, chips):
                        k_pos = k_pos + jnp.where(col >= k * r, r, 0)
                    weights = jnp.where(k_pos <= q_pos, weights, 0.0)
                total = total + dot(weights.astype(bf16), values[h, cols, :])
            acc[h, at, :] = total

    def all_rows(masked):
        def one(i, _):
            accumulate(i, masked)
            return 0

        lax.fori_loop(0, chips, one, 0)

    def block_of(j):
        odd = lax.rem(j, 2)
        jj = jnp.where(side == 1, j, j - 1 + 2 * odd)
        return shard - jj, 1 - lax.rem(jj, 2)

    def forward(j):
        block, mine = block_of(j)
        arrived(piece(block, core), d_recv.at[block, core])

        @pl.when((mine == 1) & (deep < last_deep))
        def _():
            onward(block).start()

        @pl.when(mine == 1)
        def _():
            across(block).start()

        near(block).start()

    def ready(j):
        block, _ = block_of(j)
        arrived(piece(block, 1 - core), d_recv.at[block, 1 - core])
        prepare(block)

    def one_block(j, _):
        forward(j)

        @pl.when(j > 1)
        def _():
            ready(j - 1)
            all_rows(False)

        return 0

    @pl.when(shard > 0)
    def _():
        arrived(pool_ext.at[pl.ds(0, RIM), :], p_recv)

    def pool(i, _):
        base = pl.multiple_of(i * LANES, LANES)
        ext = pool_ext[pl.ds(base, LANES + RIM), :].astype(f32)
        channel = me * pc + lax.broadcasted_iota(jnp.int32, (LANES, pc), 1)
        window = jnp.left_shift(jnp.int32(2), lax.div(channel, GROUP))
        total = ext
        chosen = None
        for level in range(4):
            total = total + pltpu.roll(total, 1 << level, 0)
            if chosen is None:
                chosen = total[RIM:]
            else:
                chosen = jnp.where(window >= (2 << level), total[RIM:], chosen)
        position = shard * rows + base + lax.broadcasted_iota(jnp.int32, (LANES, pc), 0)
        divisor = jnp.minimum(position + 1, window).astype(f32)
        pooled = (chosen / divisor - ext[RIM:]) * pool_gain[...]
        act[pl.ds(base, LANES), :pc] = pooled.astype(bf16)
        return 0

    lax.fori_loop(0, rows // LANES, pool, 0)

    lax.fori_loop(1, shard + 1, one_block, 0)

    arrived(piece(shard, 1 - core), d_recv.at[shard, 1 - core])
    prepare(shard)
    all_rows(True)

    @pl.when(shard > 0)
    def _():
        ready(shard)

        def one(step, _):
            accumulate(lax.rem(chip + step, chips), False)
            return 0

        lax.fori_loop(1, chips, one, 0)

    def finish(k):
        at = pl.ds(pl.multiple_of(k * q_tile, q_tile), q_tile)
        parts = []
        for h in range(heads):
            a = acc[h, at, :]
            parts.append(a[:, :VDIM] / a[:, VDIM : VDIM + 1])
        act[at, pc:] = jnp.concatenate(parts, axis=1).astype(bf16)
        copy = remote(
            act.at[rows_at(place(k, 1 - core), 0, r), :], act_p.at[k], act_send.at[k], act_recv.at[k], {"tp": partner}
        )
        copy.start()
        sends.append(copy)

    cw = width // COLS

    def product(k, n):
        cols = pl.ds(n * cw, cw)
        mine = act[rows_at(place(k, core), 0, r), :]
        return dot(mine, wo[:, cols]) + dot(act_p[k], wo_p[:, cols])

    for step in range(1, chips):
        finish(ahead(step))
    arrived(wo_p, wo_recv)
    for step in range(1, chips):
        k = ahead(step)
        arrived(act_p.at[k], act_recv.at[k])
        for n in range(COLS):
            f_out[step - 1, n] = product(k, n).astype(bf16)
            copy = remote(
                f_out.at[step - 1, n],
                f_in.at[step - 1, n],
                f_send.at[step - 1, n],
                f_recv.at[step - 1, n],
                {"tp": place(k, core)},
            )
            copy.start()
            sends.append(copy)

    @pl.when(shard > 0)
    def _():
        accumulate(chip, False)

    finish(chip)
    arrived(act_p.at[chip], act_recv.at[chip])
    for n in range(COLS):
        total = product(chip, n)
        for step in range(1, chips):
            arrived(f_in.at[step - 1, n], f_recv.at[step - 1, n])
            total = total + f_in[step - 1, n].astype(f32)
        out_ref[:, n * cw : (n + 1) * cw] = total.astype(bf16)

    for copy in sends:
        copy.wait_send()
    wo_copy.wait_send()

    @pl.when(shard < n_sp - 1)
    def _():
        rim_copy.wait_send()

    def drain(j, _):
        block = shard - j
        near(block).wait_send()

        @pl.when((lax.rem(j, 2) == 0) & (deep < last_deep))
        def _():
            onward(block).wait_send()

        @pl.when((lax.rem(j, 2) == 0) & ((j > 0) | (side == 0)))
        def _():
            across(block).wait_send()

        return 0

    lax.fori_loop(0, shard + 1, drain, 0)


def tables(n_sp, n_tp, rows):
    frequency = np.float32(rope_theta) ** (-np.arange(0, ROPE, 2, dtype=np.float32) / np.float32(ROPE))
    r = rows // n_tp

    def make(positions):
        angles = frequency.astype(np.float32)[:, None] * positions.astype(np.float32)[None, :]
        angles = angles.astype(np.float64)
        return np.cos(angles).astype(np.float32), np.sin(angles).astype(np.float32)

    natural = np.arange(rows)
    split = natural.reshape(n_tp // 2, 2, r).transpose(1, 0, 2).reshape(-1)
    blocks = make(np.arange(n_sp) * rows)
    columns = [np.ascontiguousarray(t.T)[:, :, None] for t in blocks]
    return [*make(natural), *make(split), *columns]


def local(
    activations,
    in_gain,
    w_pool_in,
    pool_gain,
    w_qlat,
    w_kvlat,
    w_krope,
    qlat_gain,
    kvlat_gain,
    w_qup,
    w_kup,
    w_vup,
    qhead_gain,
    khead_gain,
    w_out_pool,
    w_out_attn,
):
    n_sp, n_tp = lax.axis_size("sp"), lax.axis_size("tp")
    r, width = activations.shape
    rows, chips = r * n_tp, n_tp // 2
    half = r * chips
    others = max(1, chips - 1)
    qc, kc, pc = w_qlat.shape[1], w_kvlat.shape[1], w_pool_in.shape[1]
    heads = w_kup.shape[1] // NOPE
    kvlat = w_kup.shape[0]
    hc = heads * VDIM
    qp = up_to(qc, LANES)
    vm = pl.BlockSpec(memory_space=pltpu.VMEM)
    hbm = pl.BlockSpec(memory_space=pl.ANY)
    scratch = [
        ((r, width), bf16),
        ((width, pc), bf16),
        ((width, qc), bf16),
        ((width, kc), bf16),
        (w_krope.shape, bf16),
        (w_qup.shape, bf16),
        (w_kup.shape, bf16),
        (w_vup.shape, bf16),
        ((pc + hc, width), bf16),
        ((pc + hc, width), bf16),
        ((width, qp), bf16),
        ((width, 2 * LANES), bf16),
        ((n_tp, heads * HEAD, qp), bf16),
        ((heads * NOPE, kvlat), bf16),
        ((kvlat, heads * LANES), bf16),
        ((n_tp, r, width), bf16),
        ((n_tp, rows, qp), bf16),
        ((2, chips, r, kc), bf16),
        ((n_tp, chips, r, kc), bf16),
        ((half, LANES), f32),
        ((n_sp, 2, half + ROPE, kvlat), bf16),
        ((rows + RIM, pc), bf16),
        ((heads, rows, LANES), bf16),
        ((heads, LANES, rows), bf16),
        ((heads, rows, LANES), bf16),
        ((heads, rows, LANES), f32),
        ((rows, pc + hc), bf16),
        ((chips, r, pc + hc), bf16),
        ((others, COLS, r, width // COLS), bf16),
        ((others, COLS, r, width // COLS), bf16),
    ]
    dma = pltpu.SemaphoreType.DMA
    sems = [
        (10,),
        (others, CHUNKS),
        (CHUNKS,),
        (others, CHUNKS),
        (n_tp, CHUNKS),
        (n_tp,),
        (n_tp,),
        (others,),
        None,
        (others,),
        (n_tp,),
        (n_sp,),
        (n_sp,),
        (n_sp,),
        (n_sp, 2),
        None,
        None,
        None,
        None,
        (chips,),
        (chips,),
        (others, COLS),
        (others, COLS),
    ]
    small = [
        in_gain.reshape(1, -1),
        pool_gain.reshape(1, -1),
        qlat_gain.reshape(-1, 1),
        kvlat_gain.reshape(1, -1),
        qhead_gain.reshape(-1, 1),
        khead_gain.reshape(-1, 1),
    ] + [jnp.asarray(t) for t in tables(n_sp, n_tp, rows)]
    return pl.pallas_call(
        functools.partial(mixer_kernel, n_sp, n_tp),
        out_shape=jax.ShapeDtypeStruct((r, width), bf16),
        in_specs=[hbm] * 10 + [vm] * len(small),
        out_specs=vm,
        scratch_shapes=[pltpu.VMEM(s, d) for s, d in scratch] + [dma if s is None else dma(s) for s in sems],
        compiler_params=pltpu.CompilerParams(
            collective_id=0, has_side_effects=True, vmem_limit_bytes=67_043_328
        ),
    )(
        activations,
        w_pool_in,
        w_qlat,
        w_kvlat,
        w_krope,
        w_qup,
        w_kup,
        w_vup,
        w_out_pool,
        w_out_attn,
        *small,
    )


def solution(mesh):
    placed = (
        P(("sp", "tp"), None),
        P(),
        P(None, "tp"),
        P("tp"),
        P(None, "tp"),
        P(None, "tp"),
        P(),
        P(),
        P(),
        P(None, "tp"),
        P(None, "tp"),
        P(None, "tp"),
        P(),
        P(),
        P("tp", None),
        P("tp", None),
    )
    return jax.shard_map(
        local, mesh=mesh, in_specs=placed, out_specs=P(("sp", "tp"), None), check_vma=False
    )
```

```python
import functools
import math

import jax
import jax.numpy as jnp
import numpy as np
from jax import lax
from jax.experimental import pallas as pl
from jax.experimental.pallas import tpu as pltpu
from jax.sharding import PartitionSpec as P

GROUP = 256
NOPE = 64
ROPE = 32
VDIM = 64
HEAD = NOPE + ROPE
HALF = ROPE // 2
LANES = 128
RIM = 16
CHUNKS = 3
COLS = 4
VMEM_MOST = 67_043_328
SPARE = 6 * 1024 * 1024

norm_eps = 1e-06
rope_theta = 10000.0
bf16 = jnp.bfloat16
f32 = jnp.float32
MESH = pl.DeviceIdType.MESH
NT = (((1,), (1,)), ((), ()))


def up_to(n, m):
    return (n + m - 1) // m * m


def dot(a, b):
    return jnp.dot(a, b, preferred_element_type=f32)


def dot_nt(a, b):
    return lax.dot_general(a, b, NT, preferred_element_type=f32)


def remote(src, dst, send_sem, recv_sem, target):
    return pltpu.make_async_remote_copy(
        src_ref=src, dst_ref=dst, send_sem=send_sem, recv_sem=recv_sem, device_id=target, device_id_type=MESH
    )


def padded_transpose(w):
    rows, cols = w.shape
    r, c = up_to(rows, LANES), up_to(cols, LANES)
    w = w.astype(f32)
    if r > rows:
        w = jnp.concatenate([w, jnp.zeros((r - rows, cols), f32)], axis=0)
    if c > cols:
        w = jnp.concatenate([w, jnp.zeros((r, c - cols), f32)], axis=1)
    return w.T[:cols]


def column(row):
    count = row.shape[1]
    wide = up_to(count, LANES)
    if wide > count:
        row = jnp.concatenate([row, jnp.zeros((1, wide - count), f32)], axis=1)
    return jnp.broadcast_to(row, (LANES, wide)).T[:count]


def mixer_kernel(
    n_sp,
    n_tp,
    keep,
    x_hbm,
    wpool_hbm,
    wq_hbm,
    wkv_hbm,
    wkr_hbm,
    wqup_hbm,
    wkup_hbm,
    wvup_hbm,
    wop_hbm,
    woa_hbm,
    in_gain_hbm,
    pool_gain_hbm,
    qlat_gain_hbm,
    kvlat_gain_hbm,
    qh_gain_hbm,
    kh_gain_hbm,
    cos_q_hbm,
    sin_q_hbm,
    cos_k_hbm,
    sin_k_hbm,
    cos_b_hbm,
    sin_b_hbm,
    out_ref,
    in_gain,
    pool_gain,
    qlat_gain,
    kvlat_gain,
    qh_gain,
    kh_gain,
    cos_q,
    sin_q,
    cos_k,
    sin_k,
    cos_b,
    sin_b,
    x_own,
    wpool,
    wq_raw,
    wkv_raw,
    wkr_raw,
    wqup,
    wkup,
    wvup,
    wo,
    wo_p,
    wq_cat,
    wkv_cat,
    wq_t,
    wk_t,
    wv_pad,
    gain_q,
    gain_k,
    xg,
    qx,
    kv_mine,
    kvx,
    rope_own,
    kv_all,
    pool_ext,
    queries,
    keys_t,
    values,
    acc,
    act,
    act_p,
    f_out,
    f_in,
    ld_sem,
    a_far_send,
    a_near_send,
    a_relay_send,
    a_recv,
    kv_send,
    kv_recv,
    q_far_send,
    q_near_send,
    q_relay_send,
    q_recv,
    up_send,
    side_send,
    near_send,
    d_recv,
    p_send,
    p_recv,
    wo_send,
    wo_recv,
    act_send,
    act_recv,
    f_send,
    f_recv,
):
    me = lax.axis_index("tp")
    core, chip = lax.rem(me, 2), lax.div(me, 2)
    chips = n_tp // 2
    partner = me + 1 - 2 * core
    shard = lax.axis_index("sp")
    deep, side = lax.div(shard, 2), lax.rem(shard, 2)
    last_deep = n_sp // 2 - 1
    other = shard + 1 - 2 * side

    r, width = x_own.shape
    rows = r * n_tp
    half = r * chips
    qc = wq_raw.shape[0]
    kc = wkv_raw.shape[1]
    kvlat = kc * n_tp
    pc = wpool.shape[1]
    heads = wkup.shape[1] // NOPE
    hc = heads * VDIM
    rc = r // CHUNKS

    loads = {}

    def load(i, name, src, dst):
        loads[name] = pltpu.make_async_copy(src, dst, ld_sem.at[i])
        loads[name].start()

    load(0, "x", x_hbm, x_own)
    load(10, "in_gain", in_gain_hbm, in_gain)
    load(1, "wkv", wkv_hbm, wkv_raw)
    load(2, "wkr", wkr_hbm, wkr_raw)
    load(3, "wq", wq_hbm, wq_raw)
    load(4, "wpool", wpool_hbm, wpool)
    load(5, "wqup", wqup_hbm, wqup)
    load(6, "wkup", wkup_hbm, wkup)
    load(7, "wvup", wvup_hbm, wvup)
    load(8, "wop", wop_hbm, wo.at[pl.ds(0, pc), :])
    load(9, "woa", woa_hbm, wo.at[pl.ds(pc, hc), :])
    small = {
        "pool_gain": (pool_gain_hbm, pool_gain),
        "qlat_gain": (qlat_gain_hbm, qlat_gain),
        "kvlat_gain": (kvlat_gain_hbm, kvlat_gain),
        "qh_gain": (qh_gain_hbm, qh_gain),
        "kh_gain": (kh_gain_hbm, kh_gain),
        "cos_q": (cos_q_hbm, cos_q),
        "sin_q": (sin_q_hbm, sin_q),
        "cos_k": (cos_k_hbm, cos_k),
        "sin_k": (sin_k_hbm, sin_k),
        "cos_b": (cos_b_hbm, cos_b),
        "sin_b": (sin_b_hbm, sin_b),
    }
    for i, (name, pair) in enumerate(small.items()):
        load(11 + i, name, *pair)

    barrier = pltpu.get_barrier_semaphore()
    for step in range(1, n_tp):
        pl.semaphore_signal(
            barrier, inc=1, device_id={"tp": lax.rem(me + step, n_tp)}, device_id_type=MESH
        )
    greeted = n_tp - 1
    for gap in (-2, -1, 1, 2):
        there = shard + gap
        valid = (there >= 0) & (there < n_sp)

        @pl.when(valid)
        def _():
            pl.semaphore_signal(barrier, inc=1, device_id={"sp": there}, device_id_type=MESH)

        greeted = greeted + jnp.where(valid, 1, 0)
    pl.semaphore_wait(barrier, greeted)

    def place(k, c):
        return 2 * k + c

    def behind(step):
        return lax.rem(chip + chips - step, chips)

    def ahead(step):
        return lax.rem(chip + step, chips)

    def rows_at(g, off, count):
        return pl.ds(pl.multiple_of(g * r + off, 16), count)

    def arrived(ref, sem):
        remote(ref, ref, a_near_send.at[0], sem, {"tp": partner}).wait_recv()

    sends = []
    loads["x"].wait()
    loads["in_gain"].wait()
    for c in range(CHUNKS):
        at = pl.ds(c * rc, rc)
        xf = x_own[at, :].astype(f32)
        factor = lax.rsqrt(jnp.mean(xf * xf, axis=1, keepdims=True) + norm_eps)
        xg[me, at, :] = (xf * factor * in_gain[...]).astype(bf16)
        own = xg.at[me, at, :]
        for step in range(1, chips):
            copy = remote(
                own, own, a_far_send.at[step - 1, c], a_recv.at[me, c], {"tp": place(ahead(step), core)}
            )
            copy.start()
            sends.append(copy)
    for c in range(CHUNKS):
        own = xg.at[me, pl.ds(c * rc, rc), :]
        copy = remote(own, own, a_near_send.at[c], a_recv.at[me, c], {"tp": partner})
        copy.start()
        sends.append(copy)

    loads["wkv"].wait()
    loads["wkr"].wait()
    wkv_cat[:, :kc] = wkv_raw[...]
    wkv_cat[:, LANES:] = padded_transpose(wkr_raw[...]).astype(bf16)
    loads["wq"].wait()
    wq_cat[...] = padded_transpose(wq_raw[...]).astype(bf16)
    loads["wpool"].wait()

    def project(k, c, off, count, same_core):
        g = place(k, c)
        xs = xg[g, pl.ds(off, count), :]
        at = rows_at(g, off, count)
        both = dot(xs, wkv_cat[...])
        kv_mine[c, k, pl.ds(off, count), :] = both[:, :kc].astype(bf16)
        if same_core:
            shared = both[:, LANES : 2 * LANES].astype(bf16).astype(f32)
            rope_own[pl.ds(pl.multiple_of(k * r + off, 8), count), :] = shared
        qx[me, at, :] = dot(xs, wq_cat[...]).astype(bf16)
        at_ext = pl.ds(pl.multiple_of(g * r + off + RIM, 16), count)
        pool_ext[at_ext, :] = dot(xs, wpool[...]).astype(bf16)

    project(chip, core, 0, r, True)
    for c in range(CHUNKS):
        arrived(xg.at[partner, pl.ds(c * rc, rc), :], a_recv.at[partner, c])
    project(chip, 1 - core, 0, r, False)

    loads["wqup"].wait()
    for name in small:
        loads[name].wait()
    lat_rows = qlat_gain[...]
    lat_gain = jnp.concatenate([column(lat_rows[i : i + 1]) for i in range(lat_rows.shape[0])], axis=0)
    gain_q[...] = column(qh_gain[...])
    gain_k[...] = column(kh_gain[...])
    for src in range(n_tp):
        span = slice(src * qc, (src + 1) * qc)
        part = wqup[span, :].astype(f32) * lat_gain[span, :1]
        wq_t[src] = padded_transpose(part).astype(bf16)
    loads["wkup"].wait()
    wk_t[...] = padded_transpose(wkup[...]).astype(bf16)
    loads["wvup"].wait()
    wv_pad[...] = jnp.zeros_like(wv_pad)
    for h in range(heads):
        wv_pad[:, h * LANES : h * LANES + VDIM] = (
            wvup[...].astype(f32)[:, h * VDIM : (h + 1) * VDIM].astype(bf16)
        )
    acc[...] = jnp.zeros_like(acc)

    loads["wop"].wait()
    loads["woa"].wait()
    wo_copy = remote(wo, wo_p, wo_send, wo_recv, {"tp": partner})
    wo_copy.start()

    for c in range(CHUNKS):
        at = pl.ds(c * rc, rc)
        for step in range(1, chips):
            g = place(behind(step), core)
            block = xg.at[g, at, :]
            arrived(block, a_recv.at[g, c])
            copy = remote(block, block, a_relay_send.at[step - 1, c], a_recv.at[g, c], {"tp": partner})
            copy.start()
            sends.append(copy)
        for step in range(1, chips):
            project(behind(step), core, c * rc, rc, True)
        for step in range(1, chips):
            g = place(behind(step), 1 - core)
            arrived(xg.at[g, at, :], a_recv.at[g, c])
            project(behind(step), 1 - core, c * rc, rc, False)

    for step in range(1, n_tp):
        there = lax.rem(me + step, n_tp)
        copy = remote(
            kv_mine.at[lax.rem(there, 2)], kvx.at[me], kv_send.at[step - 1], kv_recv.at[me], {"tp": there}
        )
        copy.start()
        sends.append(copy)
    own_q = qx.at[me]
    for step in range(1, chips):
        copy = remote(own_q, own_q, q_far_send.at[step - 1], q_recv.at[me], {"tp": place(ahead(step), core)})
        copy.start()
        sends.append(copy)
    copy = remote(own_q, own_q, q_near_send, q_recv.at[me], {"tp": partner})
    copy.start()
    sends.append(copy)

    rim_copy = remote(
        pool_ext.at[pl.ds(rows, RIM), :], pool_ext.at[pl.ds(0, RIM), :], p_send, p_recv, {"sp": shard + 1}
    )

    @pl.when(shard < n_sp - 1)
    def _():
        rim_copy.start()

    @pl.when(shard == 0)
    def _():
        pool_ext[pl.ds(0, RIM), :] = jnp.zeros((RIM, pc), bf16)

    kvx[me] = kv_mine[core]
    for step in range(1, n_tp):
        source = lax.rem(me + step, n_tp)
        arrived(kvx.at[source], kv_recv.at[source])
    lat = jnp.concatenate([kvx[i].reshape(half, kc).astype(f32) for i in range(n_tp)], axis=1)
    factor = lax.rsqrt(jnp.mean(lat * lat, axis=1, keepdims=True) + norm_eps)
    kv_all[shard, core, pl.ds(0, half), :] = (lat * factor * kvlat_gain[...]).astype(bf16)
    kv_all[shard, core, pl.ds(half, ROPE), pl.ds(0, half)] = rope_own[...].T[:ROPE].astype(bf16)

    def piece(block, h):
        return kv_all.at[block, h]

    def onward(block):
        return remote(
            piece(block, core), piece(block, core), up_send.at[block], d_recv.at[block, core], {"sp": shard + 2}
        )

    def across(block):
        return remote(
            piece(block, core), piece(block, core), side_send.at[block], d_recv.at[block, core], {"sp": other}
        )

    def near(block):
        return remote(
            piece(block, core), piece(block, core), near_send.at[block], d_recv.at[block, core], {"tp": partner}
        )

    @pl.when(deep < last_deep)
    def _():
        onward(shard).start()

    @pl.when(side == 0)
    def _():
        across(shard).start()

    near(shard).start()

    score_scale = HEAD ** (-0.5) * math.log2(math.e)
    q_tile = 2 * r

    def table(cos_ref, sin_ref, block, at):
        ca, sa = cos_ref[:, at], sin_ref[:, at]
        cb, sb = cos_b[block], sin_b[block]
        return ca * cb - sa * sb, sa * cb + ca * sb

    def make_queries(i, _):
        at = pl.ds(pl.multiple_of(i * half, half), half)
        raw = None
        squares = None
        ones = jnp.ones((8, qx.shape[2]), bf16)
        for src in range(n_tp):
            part = qx[src, at, :]
            term = dot_nt(wq_t[src], part)
            raw = term if raw is None else raw + term
            pf = part.astype(f32)
            term = dot_nt(ones, (pf * pf).astype(bf16))
            squares = term if squares is None else squares + term
        eps = norm_eps * (squares[:1] * (1.0 / (qc * n_tp)) + norm_eps)
        cosine, sine = table(cos_q, sin_q, shard, at)
        for h in range(heads):
            x = raw[h * HEAD : (h + 1) * HEAD]
            factor = lax.rsqrt(jnp.sum(x * x, axis=0, keepdims=True) * (1.0 / HEAD) + eps) * score_scale
            y = x * factor * gain_q[:, :1]
            low, high = y[NOPE : NOPE + HALF], y[NOPE + HALF :]
            full = jnp.concatenate(
                [
                    y[:NOPE] * gain_k[:NOPE, :1],
                    low * cosine - high * sine,
                    high * cosine + low * sine,
                    jnp.zeros((LANES - HEAD, half), f32),
                ],
                axis=0,
            )
            queries[h, at, :] = full.T.astype(bf16)
        return 0


    lane = lax.broadcasted_iota(jnp.int32, (half, LANES), 1)

    def prepare(block):
        slot = block if keep else 0
        for c in range(2):
            at = pl.ds(c * half, half)
            lat = kv_all[block, c, pl.ds(0, half), :]
            shared = kv_all[block, c, pl.ds(half, ROPE), pl.ds(0, half)].astype(f32)
            shared_sq = jnp.sum(shared * shared, axis=0, keepdims=True)
            cosine, sine = table(cos_k, sin_k, block, at)
            gained = shared * gain_k[NOPE:, :1]
            low, high = gained[:HALF], gained[HALF:]
            turned = jnp.concatenate([low * cosine - high * sine, high * cosine + low * sine], axis=0)
            plain = dot_nt(wk_t[...], lat)
            value = dot(lat, wv_pad[...])
            for h in range(heads):
                x = plain[h * NOPE : (h + 1) * NOPE]
                total = jnp.sum(x * x, axis=0, keepdims=True) + shared_sq
                factor = lax.rsqrt(total * (1.0 / HEAD) + norm_eps)
                keys_t[slot, h, :NOPE, at] = (x * factor).astype(bf16)
                keys_t[slot, h, NOPE:HEAD, at] = (turned * factor).astype(bf16)
                keys_t[slot, h, HEAD:, at] = jnp.zeros((LANES - HEAD, half), bf16)
                v = jnp.where(lane == VDIM, 1.0, value[:, h * LANES : (h + 1) * LANES])
                values[slot, h, at, :] = v.astype(bf16)

    key_tile = math.gcd(half, 384)

    def accumulate(block, i, masked):
        slot = block if keep else 0
        at = pl.ds(pl.multiple_of(i * q_tile, q_tile), q_tile)
        for h in range(heads):
            q = queries[h, at, :]
            total = acc[h, at, :]
            for j in range(rows // key_tile):
                cols = pl.ds(j * key_tile, key_tile)
                weights = jnp.exp2(dot(q, keys_t[slot, h, :, cols]))
                if masked:
                    q_pos = i * q_tile + lax.broadcasted_iota(jnp.int32, weights.shape, 0)
                    col = (j * key_tile) % half + lax.broadcasted_iota(jnp.int32, weights.shape, 1)
                    k_pos = col + ((j * key_tile) // half) * r
                    for k in range(1, chips):
                        k_pos = k_pos + jnp.where(col >= k * r, r, 0)
                    weights = jnp.where(k_pos <= q_pos, weights, 0.0)
                total = total + dot(weights.astype(bf16), values[slot, h, cols, :])
            acc[h, at, :] = total

    def far_rows(block, masked):
        def one(step, _):
            accumulate(block, lax.rem(chip + step, chips), masked)
            return 0

        lax.fori_loop(1, chips, one, 0)

    def early_rows(block, masked):
        far_rows(block, masked)
        if not keep:
            accumulate(block, chip, masked)

    def z_block(e):
        return shard - 2 * e

    def y_block(e):
        return other - 2 * (e - 1)

    def y_valid(e):
        return (e - 1 >= 1 - side) & (e - 1 <= deep)

    def forward(e):
        @pl.when(e <= deep)
        def _():
            block = z_block(e)
            arrived(piece(block, core), d_recv.at[block, core])

            @pl.when(deep < last_deep)
            def _():
                onward(block).start()

            across(block).start()
            near(block).start()

        @pl.when(y_valid(e))
        def _():
            block = y_block(e)
            arrived(piece(block, core), d_recv.at[block, core])
            near(block).start()

    def ready(block):
        arrived(piece(block, 1 - core), d_recv.at[block, 1 - core])
        prepare(block)

    @pl.when(shard > 0)
    def _():
        arrived(pool_ext.at[pl.ds(0, RIM), :], p_recv)

    def pool(i, _):
        base = pl.multiple_of(i * LANES, LANES)
        ext = pool_ext[pl.ds(base, LANES + RIM), :].astype(f32)
        channel = me * pc + lax.broadcasted_iota(jnp.int32, (LANES, pc), 1)
        window = jnp.left_shift(jnp.int32(2), lax.div(channel, GROUP))
        total = ext
        chosen = None
        for level in range(4):
            total = total + pltpu.roll(total, 1 << level, 0)
            if chosen is None:
                chosen = total[RIM:]
            else:
                chosen = jnp.where(window >= (2 << level), total[RIM:], chosen)
        position = shard * rows + base + lax.broadcasted_iota(jnp.int32, (LANES, pc), 0)
        divisor = jnp.minimum(position + 1, window).astype(f32)
        pooled = (chosen / divisor - ext[RIM:]) * pool_gain[...]
        act[pl.ds(base, LANES), :pc] = pooled.astype(bf16)
        return 0

    lax.fori_loop(0, rows // LANES, pool, 0)

    forward(1)

    for step in range(1, chips):
        g = place(behind(step), core)
        arrived(qx.at[g], q_recv.at[g])
        copy = remote(qx.at[g], qx.at[g], q_relay_send.at[step - 1], q_recv.at[g], {"tp": partner})
        copy.start()
        sends.append(copy)
    for k in range(chips):
        g = place(k, 1 - core)
        arrived(qx.at[g], q_recv.at[g])

    lax.fori_loop(0, 2, make_queries, 0)

    ready(shard)
    early_rows(shard, True)

    def reach(e):
        return jnp.minimum(2 * deep, jnp.where(e == 1, 0, jnp.where(e == 2, 3, 2 * e)))

    def one_event(e, _):
        forward(e)

        def one(i, _):
            k = lax.div(i + 1, 2)
            first = lax.rem(i, 2) == 1
            block = jnp.where(first, z_block(k), y_block(k))

            @pl.when(first | y_valid(k))
            def _():
                ready(block)
                early_rows(block, False)

            return 0

        lax.fori_loop(reach(e - 1) + 1, reach(e) + 1, one, 0)
        return 0

    lax.fori_loop(2, deep + 2, one_event, 0)
    final = y_block(deep + 1)
    has_final = y_valid(deep + 1)

    @pl.when(has_final)
    def _():
        ready(final)
        far_rows(final, False)

    def finish(k):
        at = pl.ds(pl.multiple_of(k * q_tile, q_tile), q_tile)
        parts = []
        for h in range(heads):
            a = acc[h, at, :]
            parts.append(a[:, :VDIM] / a[:, VDIM : VDIM + 1])
        act[at, pc:] = jnp.concatenate(parts, axis=1).astype(bf16)
        copy = remote(
            act.at[rows_at(place(k, 1 - core), 0, r), :], act_p.at[k], act_send.at[k], act_recv.at[k], {"tp": partner}
        )
        copy.start()
        sends.append(copy)

    cw = width // COLS

    def product(k, n):
        cols = pl.ds(n * cw, cw)
        mine = act[rows_at(place(k, core), 0, r), :]
        return dot(mine, wo[:, cols]) + dot(act_p[k], wo_p[:, cols])

    for step in range(1, chips):
        finish(ahead(step))
    arrived(wo_p, wo_recv)
    for step in range(1, chips):
        k = ahead(step)
        arrived(act_p.at[k], act_recv.at[k])
        for n in range(COLS):
            f_out[step - 1, n] = product(k, n).astype(bf16)
            copy = remote(
                f_out.at[step - 1, n],
                f_in.at[step - 1, n],
                f_send.at[step - 1, n],
                f_recv.at[step - 1, n],
                {"tp": place(k, core)},
            )
            copy.start()
            sends.append(copy)

    if keep:
        accumulate(shard, chip, True)

        def own_rows(block, _):
            accumulate(block, chip, False)
            return 0

        lax.fori_loop(0, shard, own_rows, 0)
    else:

        @pl.when(has_final)
        def _():
            accumulate(final, chip, False)

    finish(chip)
    arrived(act_p.at[chip], act_recv.at[chip])
    for n in range(COLS):
        total = product(chip, n)
        for step in range(1, chips):
            arrived(f_in.at[step - 1, n], f_recv.at[step - 1, n])
            total = total + f_in[step - 1, n].astype(f32)
        out_ref[:, n * cw : (n + 1) * cw] = total.astype(bf16)

    for copy in sends:
        copy.wait_send()
    wo_copy.wait_send()

    @pl.when(shard < n_sp - 1)
    def _():
        rim_copy.wait_send()

    def drain(j, _):
        block = shard - j
        near(block).wait_send()

        @pl.when((lax.rem(j, 2) == 0) & (deep < last_deep))
        def _():
            onward(block).wait_send()

        @pl.when((lax.rem(j, 2) == 0) & ((j > 0) | (side == 0)))
        def _():
            across(block).wait_send()

        return 0

    lax.fori_loop(0, shard + 1, drain, 0)


def vmem_bytes(arrays):
    total = 0
    for shape, kind in arrays:
        size = 2 if kind == bf16 else 4
        minor = up_to(shape[-1], LANES) * up_to(shape[-2], 32 // size) * size
        total += math.prod(shape[:-2]) * minor
    return total


def tables(n_sp, n_tp, rows):
    frequency = np.float32(rope_theta) ** (-np.arange(0, ROPE, 2, dtype=np.float32) / np.float32(ROPE))
    r = rows // n_tp

    def make(positions):
        angles = frequency.astype(np.float32)[:, None] * positions.astype(np.float32)[None, :]
        angles = angles.astype(np.float64)
        return np.cos(angles).astype(np.float32), np.sin(angles).astype(np.float32)

    natural = np.arange(rows)
    split = natural.reshape(n_tp // 2, 2, r).transpose(1, 0, 2).reshape(-1)
    blocks = make(np.arange(n_sp) * rows)
    columns = [np.ascontiguousarray(t.T)[:, :, None] for t in blocks]
    return [*make(natural), *make(split), *columns]


def local(
    activations,
    in_gain,
    w_pool_in,
    pool_gain,
    w_qlat,
    w_kvlat,
    w_krope,
    qlat_gain,
    kvlat_gain,
    w_qup,
    w_kup,
    w_vup,
    qhead_gain,
    khead_gain,
    w_out_pool,
    w_out_attn,
):
    n_sp, n_tp = lax.axis_size("sp"), lax.axis_size("tp")
    r, width = activations.shape
    rows, chips = r * n_tp, n_tp // 2
    half = r * chips
    others = max(1, chips - 1)
    w_qlat, w_krope = w_qlat.T, w_krope.T
    qc, kc, pc = w_qlat.shape[0], w_kvlat.shape[1], w_pool_in.shape[1]
    heads = w_kup.shape[1] // NOPE
    kvlat = w_kup.shape[0]
    hc = heads * VDIM
    qp = up_to(qc, LANES)
    vm = pl.BlockSpec(memory_space=pltpu.VMEM)
    hbm = pl.BlockSpec(memory_space=pltpu.MemorySpace.HBM)
    small = [
        in_gain.reshape(1, -1),
        pool_gain.reshape(1, -1),
        qlat_gain.reshape(-1, LANES),
        kvlat_gain.reshape(1, -1),
        qhead_gain.reshape(1, -1),
        khead_gain.reshape(1, -1),
    ] + [jnp.asarray(t) for t in tables(n_sp, n_tp, rows)]
    def scratch_of(slots):
      return [(t.shape, f32) for t in small] + [
        ((r, width), bf16),
        ((width, pc), bf16),
        ((qc, width), bf16),
        ((width, kc), bf16),
        (w_krope.shape, bf16),
        (w_qup.shape, bf16),
        (w_kup.shape, bf16),
        (w_vup.shape, bf16),
        ((pc + hc, width), bf16),
        ((pc + hc, width), bf16),
        ((width, qp), bf16),
        ((width, 2 * LANES), bf16),
        ((n_tp, heads * HEAD, qp), bf16),
        ((heads * NOPE, kvlat), bf16),
        ((kvlat, heads * LANES), bf16),
        ((HEAD, LANES), f32),
        ((HEAD, LANES), f32),
        ((n_tp, r, width), bf16),
        ((n_tp, rows, qp), bf16),
        ((2, chips, r, kc), bf16),
        ((n_tp, chips, r, kc), bf16),
        ((half, LANES), f32),
        ((n_sp, 2, half + ROPE, kvlat), bf16),
        ((rows + RIM, pc), bf16),
        ((heads, rows, LANES), bf16),
        ((slots, heads, LANES, rows), bf16),
        ((slots, heads, rows, LANES), bf16),
        ((heads, rows, LANES), f32),
        ((rows, pc + hc), bf16),
        ((chips, r, pc + hc), bf16),
        ((others, COLS, r, width // COLS), bf16),
        ((others, COLS, r, width // COLS), bf16),
    ]
    keep = vmem_bytes(scratch_of(n_sp)) + SPARE <= VMEM_MOST
    scratch = scratch_of(n_sp if keep else 1)
    dma = pltpu.SemaphoreType.DMA
    sems = [
        (22,),
        (others, CHUNKS),
        (CHUNKS,),
        (others, CHUNKS),
        (n_tp, CHUNKS),
        (n_tp,),
        (n_tp,),
        (others,),
        None,
        (others,),
        (n_tp,),
        (n_sp,),
        (n_sp,),
        (n_sp,),
        (n_sp, 2),
        None,
        None,
        None,
        None,
        (chips,),
        (chips,),
        (others, COLS),
        (others, COLS),
    ]
    return pl.pallas_call(
        functools.partial(mixer_kernel, n_sp, n_tp, keep),
        out_shape=jax.ShapeDtypeStruct((r, width), bf16),
        in_specs=[hbm] * (10 + len(small)),
        out_specs=vm,
        scratch_shapes=[pltpu.VMEM(s, d) for s, d in scratch] + [dma if s is None else dma(s) for s in sems],
        compiler_params=pltpu.CompilerParams(
            collective_id=0, has_side_effects=True, vmem_limit_bytes=min(VMEM_MOST, vmem_bytes(scratch) + SPARE)
        ),
    )(*[pltpu.with_memory_space_constraint(t, pltpu.MemorySpace.HBM) for t in (
        activations,
        w_pool_in,
        w_qlat,
        w_kvlat,
        w_krope,
        w_qup,
        w_kup,
        w_vup,
        w_out_pool,
        w_out_attn,
        *small)]
    )


def solution(mesh):
    placed = (
        P(("sp", "tp"), None),
        P(),
        P(None, "tp"),
        P("tp"),
        P(None, "tp"),
        P(None, "tp"),
        P(),
        P(),
        P(),
        P(None, "tp"),
        P(None, "tp"),
        P(None, "tp"),
        P(),
        P(),
        P("tp", None),
        P("tp", None),
    )
    return jax.shard_map(
        local, mesh=mesh, in_specs=placed, out_specs=P(("sp", "tp"), None), check_vma=False
    )
```

```python
import functools
import math

import jax
import jax.numpy as jnp
import numpy as np
from jax import lax
from jax.experimental import pallas as pl
from jax.experimental.pallas import tpu as pltpu
from jax.sharding import PartitionSpec as P

GROUP = 256
NOPE = 64
ROPE = 32
VDIM = 64
HEAD = NOPE + ROPE
HALF = ROPE // 2
LANES = 128
RIM = 16
CHUNKS = 3
COLS = 4
VMEM_MOST = 67_043_328
SPARE = 6 * 1024 * 1024

norm_eps = 1e-06
rope_theta = 10000.0
bf16 = jnp.bfloat16
f32 = jnp.float32
MESH = pl.DeviceIdType.MESH
NT = (((1,), (1,)), ((), ()))


def up_to(n, m):
    return (n + m - 1) // m * m


def dot(a, b):
    return jnp.dot(a, b, preferred_element_type=f32)


def dot_nt(a, b):
    return lax.dot_general(a, b, NT, preferred_element_type=f32)


def remote(src, dst, send_sem, recv_sem, target):
    return pltpu.make_async_remote_copy(
        src_ref=src, dst_ref=dst, send_sem=send_sem, recv_sem=recv_sem, device_id=target, device_id_type=MESH
    )


def padded_transpose(w):
    rows, cols = w.shape
    r, c = up_to(rows, LANES), up_to(cols, LANES)
    w = w.astype(f32)
    if r > rows:
        w = jnp.concatenate([w, jnp.zeros((r - rows, cols), f32)], axis=0)
    if c > cols:
        w = jnp.concatenate([w, jnp.zeros((r, c - cols), f32)], axis=1)
    return w.T[:cols]


def column(row):
    count = row.shape[1]
    wide = up_to(count, LANES)
    if wide > count:
        row = jnp.concatenate([row, jnp.zeros((1, wide - count), f32)], axis=1)
    return jnp.broadcast_to(row, (LANES, wide)).T[:count]


def mixer_kernel(
    n_sp,
    n_tp,
    keep,
    x_hbm,
    wpool_hbm,
    wq_hbm,
    wkv_hbm,
    wkr_hbm,
    wqup_hbm,
    wkup_hbm,
    wvup_hbm,
    wop_hbm,
    woa_hbm,
    in_gain_hbm,
    pool_gain_hbm,
    qlat_gain_hbm,
    kvlat_gain_hbm,
    qh_gain_hbm,
    kh_gain_hbm,
    cos_q_hbm,
    sin_q_hbm,
    cos_k_hbm,
    sin_k_hbm,
    cos_b_hbm,
    sin_b_hbm,
    out_ref,
    in_gain,
    pool_gain,
    qlat_gain,
    kvlat_gain,
    qh_gain,
    kh_gain,
    cos_q,
    sin_q,
    cos_k,
    sin_k,
    cos_b,
    sin_b,
    x_own,
    wpool,
    wq_raw,
    wkv_raw,
    wkr_raw,
    wqup,
    wkup,
    wvup,
    wo,
    wo_p,
    wq_cat,
    wkv_cat,
    wq_t,
    wk_t,
    wv_pad,
    gain_q,
    gain_k,
    xg,
    qx,
    kv_mine,
    kvx,
    rope_own,
    kv_all,
    pool_ext,
    queries,
    keys_t,
    values,
    acc,
    act,
    act_p,
    f_out,
    f_in,
    ld_sem,
    a_far_send,
    a_near_send,
    a_relay_send,
    a_recv,
    kv_send,
    kv_recv,
    q_far_send,
    q_near_send,
    q_relay_send,
    q_recv,
    up_send,
    side_send,
    near_send,
    x_send,
    d_recv,
    p_send,
    p_recv,
    wo_send,
    wo_recv,
    act_send,
    act_recv,
    f_send,
    f_recv,
):
    me = lax.axis_index("tp")
    core, chip = lax.rem(me, 2), lax.div(me, 2)
    chips = n_tp // 2
    partner = me + 1 - 2 * core
    shard = lax.axis_index("sp")
    deep, side = lax.div(shard, 2), lax.rem(shard, 2)
    last_deep = n_sp // 2 - 1
    other = shard + 1 - 2 * side

    r, width = x_own.shape
    rows = r * n_tp
    half = r * chips
    qc = wq_raw.shape[0]
    kc = wkv_raw.shape[1]
    kvlat = kc * n_tp
    pc = wpool.shape[1]
    heads = wkup.shape[1] // NOPE
    hc = heads * VDIM
    rc = r // CHUNKS

    loads = {}

    def load(i, name, src, dst):
        loads[name] = pltpu.make_async_copy(src, dst, ld_sem.at[i])
        loads[name].start()

    load(0, "x", x_hbm, x_own)
    load(10, "in_gain", in_gain_hbm, in_gain)
    load(1, "wkv", wkv_hbm, wkv_raw)
    load(2, "wkr", wkr_hbm, wkr_raw)
    load(3, "wq", wq_hbm, wq_raw)
    load(4, "wpool", wpool_hbm, wpool)
    load(5, "wqup", wqup_hbm, wqup)
    load(6, "wkup", wkup_hbm, wkup)
    load(7, "wvup", wvup_hbm, wvup)
    load(8, "wop", wop_hbm, wo.at[pl.ds(0, pc), :])
    load(9, "woa", woa_hbm, wo.at[pl.ds(pc, hc), :])
    small = {
        "pool_gain": (pool_gain_hbm, pool_gain),
        "qlat_gain": (qlat_gain_hbm, qlat_gain),
        "kvlat_gain": (kvlat_gain_hbm, kvlat_gain),
        "qh_gain": (qh_gain_hbm, qh_gain),
        "kh_gain": (kh_gain_hbm, kh_gain),
        "cos_q": (cos_q_hbm, cos_q),
        "sin_q": (sin_q_hbm, sin_q),
        "cos_k": (cos_k_hbm, cos_k),
        "sin_k": (sin_k_hbm, sin_k),
        "cos_b": (cos_b_hbm, cos_b),
        "sin_b": (sin_b_hbm, sin_b),
    }
    for i, (name, pair) in enumerate(small.items()):
        load(11 + i, name, *pair)

    barrier = pltpu.get_barrier_semaphore()
    for step in range(1, n_tp):
        pl.semaphore_signal(
            barrier, inc=1, device_id={"tp": lax.rem(me + step, n_tp)}, device_id_type=MESH
        )
    greeted = n_tp - 1
    for gap in (-2, -1, 1, 2):
        there = shard + gap
        valid = (there >= 0) & (there < n_sp)

        @pl.when(valid)
        def _():
            pl.semaphore_signal(barrier, inc=1, device_id={"sp": there}, device_id_type=MESH)

        greeted = greeted + jnp.where(valid, 1, 0)
    pl.semaphore_wait(barrier, greeted)

    def place(k, c):
        return 2 * k + c

    def behind(step):
        return lax.rem(chip + chips - step, chips)

    def ahead(step):
        return lax.rem(chip + step, chips)

    def rows_at(g, off, count):
        return pl.ds(pl.multiple_of(g * r + off, 16), count)

    def arrived(ref, sem):
        remote(ref, ref, a_near_send.at[0], sem, {"tp": partner}).wait_recv()

    sends = []
    loads["x"].wait()
    loads["in_gain"].wait()
    for c in range(CHUNKS):
        at = pl.ds(c * rc, rc)
        xf = x_own[at, :].astype(f32)
        factor = lax.rsqrt(jnp.mean(xf * xf, axis=1, keepdims=True) + norm_eps)
        xg[me, at, :] = (xf * factor * in_gain[...]).astype(bf16)
        own = xg.at[me, at, :]
        for step in range(1, chips):
            copy = remote(
                own, own, a_far_send.at[step - 1, c], a_recv.at[me, c], {"tp": place(ahead(step), core)}
            )
            copy.start()
            sends.append(copy)
    for c in range(CHUNKS):
        own = xg.at[me, pl.ds(c * rc, rc), :]
        copy = remote(own, own, a_near_send.at[c], a_recv.at[me, c], {"tp": partner})
        copy.start()
        sends.append(copy)

    loads["wkv"].wait()
    loads["wkr"].wait()
    wkv_cat[:, :kc] = wkv_raw[...]
    wkv_cat[:, LANES:] = padded_transpose(wkr_raw[...]).astype(bf16)
    loads["wq"].wait()
    wq_cat[...] = padded_transpose(wq_raw[...]).astype(bf16)
    loads["wpool"].wait()

    def project_kv(k, c, off, count, same_core):
        both = dot(xg[place(k, c), pl.ds(off, count), :], wkv_cat[...])
        kv_mine[c, k, pl.ds(off, count), :] = both[:, :kc].astype(bf16)
        if same_core:
            shared = both[:, LANES : 2 * LANES].astype(bf16).astype(f32)
            rope_own[pl.ds(pl.multiple_of(k * r + off, 8), count), :] = shared

    def project_q(k, c, off, count):
        g = place(k, c)
        qx[me, rows_at(g, off, count), :] = dot(xg[g, pl.ds(off, count), :], wq_cat[...]).astype(bf16)

    def project_pool(k, c, off, count):
        g = place(k, c)
        at_ext = pl.ds(pl.multiple_of(g * r + off + RIM, 16), count)
        pool_ext[at_ext, :] = dot(xg[g, pl.ds(off, count), :], wpool[...]).astype(bf16)

    def project(k, c, off, count, same_core):
        project_kv(k, c, off, count, same_core)
        project_q(k, c, off, count)
        project_pool(k, c, off, count)

    def kv_piece(source, k, off, count):
        return kvx.at[source, k, pl.ds(off, count), :]

    def send_kv(k, off, count, number):
        for step in range(1, n_tp):
            there = lax.rem(me + step, n_tp)
            copy = remote(
                kv_mine.at[lax.rem(there, 2), k, pl.ds(off, count), :],
                kv_piece(me, k, off, count),
                kv_send.at[step - 1, number],
                kv_recv.at[me, number],
                {"tp": there},
            )
            copy.start()
            sends.append(copy)

    project(chip, core, 0, r, True)
    for c in range(CHUNKS):
        arrived(xg.at[partner, pl.ds(c * rc, rc), :], a_recv.at[partner, c])
    project(chip, 1 - core, 0, r, False)
    send_kv(chip, 0, r, 0)

    loads["wqup"].wait()
    for name in small:
        loads[name].wait()
    lat_rows = qlat_gain[...]
    lat_gain = jnp.concatenate([column(lat_rows[i : i + 1]) for i in range(lat_rows.shape[0])], axis=0)
    gain_q[...] = column(qh_gain[...])
    gain_k[...] = column(kh_gain[...])
    for src in range(n_tp):
        span = slice(src * qc, (src + 1) * qc)
        part = wqup[span, :].astype(f32) * lat_gain[span, :1]
        wq_t[src] = padded_transpose(part).astype(bf16)
    loads["wkup"].wait()
    wk_t[...] = padded_transpose(wkup[...]).astype(bf16)
    loads["wvup"].wait()
    wv_pad[...] = jnp.zeros_like(wv_pad)
    for h in range(heads):
        wv_pad[:, h * LANES : h * LANES + VDIM] = (
            wvup[...].astype(f32)[:, h * VDIM : (h + 1) * VDIM].astype(bf16)
        )
    acc[...] = jnp.zeros_like(acc)

    loads["wop"].wait()
    loads["woa"].wait()
    wo_copy = remote(wo, wo_p, wo_send, wo_recv, {"tp": partner})
    wo_copy.start()

    for c in range(CHUNKS):
        at = pl.ds(c * rc, rc)
        for step in range(1, chips):
            g = place(behind(step), core)
            block = xg.at[g, at, :]
            arrived(block, a_recv.at[g, c])
            copy = remote(block, block, a_relay_send.at[step - 1, c], a_recv.at[g, c], {"tp": partner})
            copy.start()
            sends.append(copy)
        for step in range(1, chips):
            project_kv(behind(step), core, c * rc, rc, True)
        if c < CHUNKS - 1:
            for step in range(1, chips):
                project_q(behind(step), core, c * rc, rc)
                project_pool(behind(step), core, c * rc, rc)
        for step in range(1, chips):
            g = place(behind(step), 1 - core)
            arrived(xg.at[g, at, :], a_recv.at[g, c])
            project_kv(behind(step), 1 - core, c * rc, rc, False)
            send_kv(behind(step), c * rc, rc, 1 + (step - 1) * CHUNKS + c)
            if c < CHUNKS - 1:
                project_q(behind(step), 1 - core, c * rc, rc)
                project_pool(behind(step), 1 - core, c * rc, rc)
    late = (CHUNKS - 1) * rc
    for step in range(1, chips):
        project_q(behind(step), core, late, rc)
        project_q(behind(step), 1 - core, late, rc)

    own_q = qx.at[me]
    for step in range(1, chips):
        copy = remote(own_q, own_q, q_far_send.at[step - 1], q_recv.at[me], {"tp": place(ahead(step), core)})
        copy.start()
        sends.append(copy)
    copy = remote(own_q, own_q, q_near_send, q_recv.at[me], {"tp": partner})
    copy.start()
    sends.append(copy)

    for step in range(1, chips):
        project_pool(behind(step), core, late, rc)
        project_pool(behind(step), 1 - core, late, rc)

    rim_copy = remote(
        pool_ext.at[pl.ds(rows, RIM), :], pool_ext.at[pl.ds(0, RIM), :], p_send, p_recv, {"sp": shard + 1}
    )

    @pl.when(shard < n_sp - 1)
    def _():
        rim_copy.start()

    @pl.when(shard == 0)
    def _():
        pool_ext[pl.ds(0, RIM), :] = jnp.zeros((RIM, pc), bf16)

    kvx[me] = kv_mine[core]
    for step in range(1, n_tp):
        source = lax.rem(me + step, n_tp)
        its_chip = lax.div(source, 2)
        arrived(kv_piece(source, its_chip, 0, r), kv_recv.at[source, 0])
        for hop in range(1, chips):
            k = lax.rem(its_chip + chips - hop, chips)
            for c in range(CHUNKS):
                number = 1 + (hop - 1) * CHUNKS + c
                arrived(kv_piece(source, k, c * rc, rc), kv_recv.at[source, number])
    p = crossed(r)

    def permuted(x):
        width = x.shape[2]
        return jnp.concatenate(
            [x[:, :p].reshape(chips * p, width), x[:, p:].reshape(chips * (r - p), width)], axis=0
        )

    lat = jnp.concatenate([permuted(kvx[i].astype(f32)) for i in range(n_tp)], axis=1)
    factor = lax.rsqrt(jnp.mean(lat * lat, axis=1, keepdims=True) + norm_eps)
    kv_all[shard, core, pl.ds(0, half), :] = (lat * factor * kvlat_gain[...]).astype(bf16)
    kv_all[shard, core, pl.ds(half, ROPE), pl.ds(0, half)] = permuted(rope_own[...].reshape(chips, r, LANES)).T[:ROPE].astype(bf16)

    tail = chips * p

    def head_rows(block, h, k):
        return kv_all.at[block, h, pl.ds(pl.multiple_of(k * p, 16), p), :]

    def tail_rows(block, h):
        return kv_all.at[block, h, pl.ds(tail, half - tail + ROPE), :]

    def parts_of(block):
        return (head_rows(block, core, chip), tail_rows(block, core))

    def to_shard(block, i, send, there):
        ref = parts_of(block)[i]
        sem = d_recv.at[block, core, chip if i == 0 else chips]
        return remote(ref, ref, send.at[block, i], sem, {"sp": there})

    def onward(block, i):
        return to_shard(block, i, up_send, shard + 2)

    def across(block, i):
        return to_shard(block, i, side_send, other)

    def over(block, step):
        ref = head_rows(block, core, chip)
        return remote(
            ref, ref, x_send.at[block, step - 1], d_recv.at[block, core, chip], {"tp": place(ahead(step), core)}
        )

    def near(block, k):
        ref = head_rows(block, core, k)
        return remote(ref, ref, near_send.at[block, k], d_recv.at[block, core, k], {"tp": partner})

    def near_tail(block):
        ref = tail_rows(block, core)
        return remote(ref, ref, near_send.at[block, chips], d_recv.at[block, core, chips], {"tp": partner})

    for i in range(2):

        @pl.when(deep < last_deep)
        def _():
            onward(shard, i).start()

        @pl.when(side == 0)
        def _():
            across(shard, i).start()

    for k in range(chips):
        near(shard, k).start()
    near_tail(shard).start()

    score_scale = HEAD ** (-0.5) * math.log2(math.e)
    q_tile = 2 * r

    def table(cos_ref, sin_ref, block, at):
        ca, sa = cos_ref[:, at], sin_ref[:, at]
        cb, sb = cos_b[block], sin_b[block]
        return ca * cb - sa * sb, sa * cb + ca * sb

    def make_queries(i, _):
        at = pl.ds(pl.multiple_of(i * half, half), half)
        raw = None
        squares = None
        ones = jnp.ones((8, qx.shape[2]), bf16)
        for src in range(n_tp):
            part = qx[src, at, :]
            term = dot_nt(wq_t[src], part)
            raw = term if raw is None else raw + term
            pf = part.astype(f32)
            term = dot_nt(ones, (pf * pf).astype(bf16))
            squares = term if squares is None else squares + term
        eps = norm_eps * (squares[:1] * (1.0 / (qc * n_tp)) + norm_eps)
        cosine, sine = table(cos_q, sin_q, shard, at)
        for h in range(heads):
            x = raw[h * HEAD : (h + 1) * HEAD]
            factor = lax.rsqrt(jnp.sum(x * x, axis=0, keepdims=True) * (1.0 / HEAD) + eps) * score_scale
            y = x * factor * gain_q[:, :1]
            low, high = y[NOPE : NOPE + HALF], y[NOPE + HALF :]
            full = jnp.concatenate(
                [
                    y[:NOPE] * gain_k[:NOPE, :1],
                    low * cosine - high * sine,
                    high * cosine + low * sine,
                    jnp.zeros((LANES - HEAD, half), f32),
                ],
                axis=0,
            )
            queries[h, at, :] = full.T.astype(bf16)
        return 0


    lane = lax.broadcasted_iota(jnp.int32, (half, LANES), 1)

    def prepare(block):
        slot = block if keep else 0
        for c in range(2):
            at = pl.ds(c * half, half)
            lat = kv_all[block, c, pl.ds(0, half), :]
            shared = kv_all[block, c, pl.ds(half, ROPE), pl.ds(0, half)].astype(f32)
            shared_sq = jnp.sum(shared * shared, axis=0, keepdims=True)
            cosine, sine = table(cos_k, sin_k, block, at)
            gained = shared * gain_k[NOPE:, :1]
            low, high = gained[:HALF], gained[HALF:]
            turned = jnp.concatenate([low * cosine - high * sine, high * cosine + low * sine], axis=0)
            plain = dot_nt(wk_t[...], lat)
            value = dot(lat, wv_pad[...])
            for h in range(heads):
                x = plain[h * NOPE : (h + 1) * NOPE]
                total = jnp.sum(x * x, axis=0, keepdims=True) + shared_sq
                factor = lax.rsqrt(total * (1.0 / HEAD) + norm_eps)
                keys_t[slot, h, :NOPE, at] = (x * factor).astype(bf16)
                keys_t[slot, h, NOPE:HEAD, at] = (turned * factor).astype(bf16)
                keys_t[slot, h, HEAD:, at] = jnp.zeros((LANES - HEAD, half), bf16)
                v = jnp.where(lane == VDIM, 1.0, value[:, h * LANES : (h + 1) * LANES])
                values[slot, h, at, :] = v.astype(bf16)

    key_tile = math.gcd(rows, 256)
    runs = key_runs(n_tp, r)

    def accumulate(block, i, masked):
        attend(block, i * q_tile, q_tile, masked)

    def attend(block, row, count, masked):
        slot = block if keep else 0
        at = pl.ds(pl.multiple_of(row, r), count)
        for h in range(heads):
            q = queries[h, at, :]
            total = acc[h, at, :]
            for j in range(rows // key_tile):
                cols = pl.ds(j * key_tile, key_tile)
                weights = jnp.exp2(dot(q, keys_t[slot, h, :, cols]))
                if masked:
                    q_pos = row + lax.broadcasted_iota(jnp.int32, weights.shape, 0)
                    col = j * key_tile + lax.broadcasted_iota(jnp.int32, weights.shape, 1)
                    k_pos = col
                    shift = 0
                    for start, first in runs:
                        if first - start != shift and start < (j + 1) * key_tile:
                            k_pos = k_pos + jnp.where(col >= start, first - start - shift, 0)
                            shift = first - start
                    weights = jnp.where(k_pos <= q_pos, weights, 0.0)
                total = total + dot(weights.astype(bf16), values[slot, h, cols, :])
            acc[h, at, :] = total

    def far_rows(block, masked):
        def one(step, _):
            accumulate(block, lax.rem(chip + step, chips), masked)
            return 0

        lax.fori_loop(1, chips, one, 0)

    def early_rows(block, masked):
        far_rows(block, masked)
        if not keep:
            accumulate(block, chip, masked)

    def z_block(e):
        return shard - 2 * e

    def y_block(e):
        return other - 2 * (e - 1)

    def y_valid(e):
        return (e - 1 >= 1 - side) & (e - 1 <= deep)

    def pass_on(block, from_z):
        for i in range(2):
            arrived(parts_of(block)[i], d_recv.at[block, core, chip if i == 0 else chips])
            if from_z:

                @pl.when(deep < last_deep)
                def _():
                    onward(block, i).start()

                across(block, i).start()
            if i == 0:
                for step in range(1, chips):
                    over(block, step).start()
                near(block, chip).start()
            else:
                near_tail(block).start()

    def forward(e):
        @pl.when(e <= deep)
        def _():
            pass_on(z_block(e), True)

        @pl.when(y_valid(e))
        def _():
            pass_on(y_block(e), False)

    def relay(block):
        for step in range(1, chips):
            k = behind(step)
            arrived(head_rows(block, core, k), d_recv.at[block, core, k])
            near(block, k).start()

    def ready(block):
        for k in range(chips):
            arrived(head_rows(block, 1 - core, k), d_recv.at[block, 1 - core, k])
        arrived(tail_rows(block, 1 - core), d_recv.at[block, 1 - core, chips])
        prepare(block)

    @pl.when(shard > 0)
    def _():
        arrived(pool_ext.at[pl.ds(0, RIM), :], p_recv)

    def pool(i, _):
        base = pl.multiple_of(i * LANES, LANES)
        ext = pool_ext[pl.ds(base, LANES + RIM), :].astype(f32)
        channel = me * pc + lax.broadcasted_iota(jnp.int32, (LANES, pc), 1)
        window = jnp.left_shift(jnp.int32(2), lax.div(channel, GROUP))
        total = ext
        chosen = None
        for level in range(4):
            total = total + pltpu.roll(total, 1 << level, 0)
            if chosen is None:
                chosen = total[RIM:]
            else:
                chosen = jnp.where(window >= (2 << level), total[RIM:], chosen)
        position = shard * rows + base + lax.broadcasted_iota(jnp.int32, (LANES, pc), 0)
        divisor = jnp.minimum(position + 1, window).astype(f32)
        pooled = (chosen / divisor - ext[RIM:]) * pool_gain[...]
        act[pl.ds(base, LANES), :pc] = pooled.astype(bf16)
        return 0

    lax.fori_loop(0, rows // LANES, pool, 0)

    forward(1)

    for step in range(1, chips):
        g = place(behind(step), core)
        arrived(qx.at[g], q_recv.at[g])
        copy = remote(qx.at[g], qx.at[g], q_relay_send.at[step - 1], q_recv.at[g], {"tp": partner})
        copy.start()
        sends.append(copy)
    for k in range(chips):
        g = place(k, 1 - core)
        arrived(qx.at[g], q_recv.at[g])

    lax.fori_loop(0, 2, make_queries, 0)

    ready(shard)
    early_rows(shard, True)

    def reach(e):
        return 2 * (e - 1)

    def one_event(e, _):
        forward(e)

        def pick(i):
            k = lax.div(i + 1, 2)
            first = lax.rem(i, 2) == 1
            return jnp.where(first, z_block(k), y_block(k)), first | y_valid(k)

        def relay_at(i):
            block, valid = pick(i)

            @pl.when(valid & (i <= reach(e)))
            def _():
                relay(block)

        def one(i, _):
            relay_at(i + 1)
            block, valid = pick(i)

            @pl.when(valid)
            def _():
                ready(block)
                early_rows(block, False)

            return 0

        relay_at(reach(e - 1) + 1)
        lax.fori_loop(reach(e - 1) + 1, reach(e) + 1, one, 0)
        return 0

    lax.fori_loop(2, deep + 2, one_event, 0)
    final = y_block(deep + 1)
    has_final = y_valid(deep + 1)

    @pl.when(has_final)
    def _():
        relay(final)
        ready(final)

    def finish(k, c):
        at = rows_at(place(k, c), 0, r)
        parts = []
        for h in range(heads):
            a = acc[h, at, :]
            parts.append(a[:, :VDIM] / a[:, VDIM : VDIM + 1])
        act[at, pc:] = jnp.concatenate(parts, axis=1).astype(bf16)

    def hand_over(k):
        finish(k, 1 - core)
        copy = remote(
            act.at[rows_at(place(k, 1 - core), 0, r), :], act_p.at[k], act_send.at[k], act_recv.at[k], {"tp": partner}
        )
        copy.start()
        sends.append(copy)

    def last_block(k, c):
        @pl.when(has_final)
        def _():
            attend(final, place(k, c) * r, r, False)

    cw = width // COLS

    def product(k, n):
        cols = pl.ds(n * cw, cw)
        mine = act[rows_at(place(k, core), 0, r), :]
        return dot(mine, wo[:, cols]) + dot(act_p[k], wo_p[:, cols])

    for step in range(1, chips):
        last_block(ahead(step), 1 - core)
        hand_over(ahead(step))
    for step in range(1, chips):
        last_block(ahead(step), core)
        finish(ahead(step), core)
    arrived(wo_p, wo_recv)
    for step in range(1, chips):
        k = ahead(step)
        arrived(act_p.at[k], act_recv.at[k])
        for n in range(COLS):
            f_out[step - 1, n] = product(k, n).astype(bf16)
            copy = remote(
                f_out.at[step - 1, n],
                f_in.at[step - 1, n],
                f_send.at[step - 1, n],
                f_recv.at[step - 1, n],
                {"tp": place(k, core)},
            )
            copy.start()
            sends.append(copy)

    if keep:
        accumulate(shard, chip, True)

        def own_rows(block, _):
            accumulate(block, chip, False)
            return 0

        lax.fori_loop(0, shard, own_rows, 0)
    else:

        @pl.when(has_final)
        def _():
            accumulate(final, chip, False)

    hand_over(chip)
    finish(chip, core)
    arrived(act_p.at[chip], act_recv.at[chip])
    for n in range(COLS):
        total = product(chip, n)
        for step in range(1, chips):
            arrived(f_in.at[step - 1, n], f_recv.at[step - 1, n])
            total = total + f_in[step - 1, n].astype(f32)
        out_ref[:, n * cw : (n + 1) * cw] = total.astype(bf16)

    for copy in sends:
        copy.wait_send()
    wo_copy.wait_send()

    @pl.when(shard < n_sp - 1)
    def _():
        rim_copy.wait_send()

    def drain(j, _):
        block = shard - j
        column = lax.rem(j, 2) == 0
        for k in range(chips):
            near(block, k).wait_send()
        near_tail(block).wait_send()

        @pl.when(j > 0)
        def _():
            for step in range(1, chips):
                over(block, step).wait_send()

        for i in range(2):

            @pl.when(column & (deep < last_deep))
            def _():
                onward(block, i).wait_send()

            @pl.when(column & ((j > 0) | (side == 0)))
            def _():
                across(block, i).wait_send()

        return 0

    lax.fori_loop(0, shard + 1, drain, 0)


def vmem_bytes(arrays):
    total = 0
    for shape, kind in arrays:
        size = 2 if kind == bf16 else 4
        minor = up_to(shape[-1], LANES) * up_to(shape[-2], 32 // size) * size
        total += math.prod(shape[:-2]) * minor
    return total


def crossed(r):
    return r * 5 // 6


def key_runs(n_tp, r):
    chips, p = n_tp // 2, crossed(r)
    runs = []
    for c in range(2):
        base = c * chips * r
        runs += [(base + k * p, (2 * k + c) * r) for k in range(chips)]
        runs += [(base + chips * p + k * (r - p), (2 * k + c) * r + p) for k in range(chips)]
    return runs


def tables(n_sp, n_tp, rows):
    frequency = np.float32(rope_theta) ** (-np.arange(0, ROPE, 2, dtype=np.float32) / np.float32(ROPE))
    r = rows // n_tp

    def make(positions):
        angles = frequency.astype(np.float32)[:, None] * positions.astype(np.float32)[None, :]
        angles = angles.astype(np.float64)
        return np.cos(angles).astype(np.float32), np.sin(angles).astype(np.float32)

    natural = np.arange(rows)
    runs = key_runs(n_tp, r) + [(rows, 0)]
    split = np.concatenate([first + np.arange(runs[i + 1][0] - at) for i, (at, first) in enumerate(runs[:-1])])
    blocks = make(np.arange(n_sp) * rows)
    columns = [np.ascontiguousarray(t.T)[:, :, None] for t in blocks]
    return [*make(natural), *make(split), *columns]


def local(
    activations,
    in_gain,
    w_pool_in,
    pool_gain,
    w_qlat,
    w_kvlat,
    w_krope,
    qlat_gain,
    kvlat_gain,
    w_qup,
    w_kup,
    w_vup,
    qhead_gain,
    khead_gain,
    w_out_pool,
    w_out_attn,
):
    n_sp, n_tp = lax.axis_size("sp"), lax.axis_size("tp")
    r, width = activations.shape
    rows, chips = r * n_tp, n_tp // 2
    half = r * chips
    others = max(1, chips - 1)
    w_qlat, w_krope = w_qlat.T, w_krope.T
    qc, kc, pc = w_qlat.shape[0], w_kvlat.shape[1], w_pool_in.shape[1]
    heads = w_kup.shape[1] // NOPE
    kvlat = w_kup.shape[0]
    hc = heads * VDIM
    qp = up_to(qc, LANES)
    vm = pl.BlockSpec(memory_space=pltpu.VMEM)
    hbm = pl.BlockSpec(memory_space=pltpu.MemorySpace.HBM)
    small = [
        in_gain.reshape(1, -1),
        pool_gain.reshape(1, -1),
        qlat_gain.reshape(-1, LANES),
        kvlat_gain.reshape(1, -1),
        qhead_gain.reshape(1, -1),
        khead_gain.reshape(1, -1),
    ] + [jnp.asarray(t) for t in tables(n_sp, n_tp, rows)]
    def scratch_of(slots):
      return [(t.shape, f32) for t in small] + [
        ((r, width), bf16),
        ((width, pc), bf16),
        ((qc, width), bf16),
        ((width, kc), bf16),
        (w_krope.shape, bf16),
        (w_qup.shape, bf16),
        (w_kup.shape, bf16),
        (w_vup.shape, bf16),
        ((pc + hc, width), bf16),
        ((pc + hc, width), bf16),
        ((width, qp), bf16),
        ((width, 2 * LANES), bf16),
        ((n_tp, heads * HEAD, qp), bf16),
        ((heads * NOPE, kvlat), bf16),
        ((kvlat, heads * LANES), bf16),
        ((HEAD, LANES), f32),
        ((HEAD, LANES), f32),
        ((n_tp, r, width), bf16),
        ((n_tp, rows, qp), bf16),
        ((2, chips, r, kc), bf16),
        ((n_tp, chips, r, kc), bf16),
        ((half, LANES), f32),
        ((n_sp, 2, half + ROPE, kvlat), bf16),
        ((rows + RIM, pc), bf16),
        ((heads, rows, LANES), bf16),
        ((slots, heads, LANES, rows), bf16),
        ((slots, heads, rows, LANES), bf16),
        ((heads, rows, LANES), f32),
        ((rows, pc + hc), bf16),
        ((chips, r, pc + hc), bf16),
        ((others, COLS, r, width // COLS), bf16),
        ((others, COLS, r, width // COLS), bf16),
    ]
    keep = vmem_bytes(scratch_of(n_sp)) + SPARE <= VMEM_MOST
    scratch = scratch_of(n_sp if keep else 1)
    dma = pltpu.SemaphoreType.DMA
    sems = [
        (22,),
        (others, CHUNKS),
        (CHUNKS,),
        (others, CHUNKS),
        (n_tp, CHUNKS),
        (n_tp, 1 + others * CHUNKS),
        (n_tp, 1 + others * CHUNKS),
        (others,),
        None,
        (others,),
        (n_tp,),
        (n_sp, 2),
        (n_sp, 2),
        (n_sp, chips + 1),
        (n_sp, others),
        (n_sp, 2, chips + 1),
        None,
        None,
        None,
        None,
        (chips,),
        (chips,),
        (others, COLS),
        (others, COLS),
    ]
    return pl.pallas_call(
        functools.partial(mixer_kernel, n_sp, n_tp, keep),
        out_shape=jax.ShapeDtypeStruct((r, width), bf16),
        in_specs=[hbm] * (10 + len(small)),
        out_specs=vm,
        scratch_shapes=[pltpu.VMEM(s, d) for s, d in scratch] + [dma if s is None else dma(s) for s in sems],
        compiler_params=pltpu.CompilerParams(
            collective_id=0, has_side_effects=True, vmem_limit_bytes=min(VMEM_MOST, vmem_bytes(scratch) + SPARE)
        ),
    )(*[pltpu.with_memory_space_constraint(t, pltpu.MemorySpace.HBM) for t in (
        activations,
        w_pool_in,
        w_qlat,
        w_kvlat,
        w_krope,
        w_qup,
        w_kup,
        w_vup,
        w_out_pool,
        w_out_attn,
        *small)]
    )


def solution(mesh):
    placed = (
        P(("sp", "tp"), None),
        P(),
        P(None, "tp"),
        P("tp"),
        P(None, "tp"),
        P(None, "tp"),
        P(),
        P(),
        P(),
        P(None, "tp"),
        P(None, "tp"),
        P(None, "tp"),
        P(),
        P(),
        P("tp", None),
        P("tp", None),
    )
    return jax.shard_map(
        local, mesh=mesh, in_specs=placed, out_specs=P(("sp", "tp"), None), check_vma=False
    )
```

```python
import functools
import math

import jax
import jax.numpy as jnp
import numpy as np
from jax import lax
from jax.experimental import pallas as pl
from jax.experimental.pallas import tpu as pltpu
from jax.sharding import PartitionSpec as P

GROUP = 256
NOPE = 64
ROPE = 32
VDIM = 64
HEAD = NOPE + ROPE
HALF = ROPE // 2
LANES = 128
RIM = 16
CHUNKS = 3
COLS = 4
VMEM_MOST = 67_043_328
SPARE = 6 * 1024 * 1024

norm_eps = 1e-06
rope_theta = 10000.0
bf16 = jnp.bfloat16
f32 = jnp.float32
MESH = pl.DeviceIdType.MESH
NT = (((1,), (1,)), ((), ()))


def up_to(n, m):
    return (n + m - 1) // m * m


def dot(a, b):
    return jnp.dot(a, b, preferred_element_type=f32)


def dot_nt(a, b):
    return lax.dot_general(a, b, NT, preferred_element_type=f32)


def remote(src, dst, send_sem, recv_sem, target):
    return pltpu.make_async_remote_copy(
        src_ref=src, dst_ref=dst, send_sem=send_sem, recv_sem=recv_sem, device_id=target, device_id_type=MESH
    )


def padded_transpose(w):
    rows, cols = w.shape
    r, c = up_to(rows, LANES), up_to(cols, LANES)
    w = w.astype(f32)
    if r > rows:
        w = jnp.concatenate([w, jnp.zeros((r - rows, cols), f32)], axis=0)
    if c > cols:
        w = jnp.concatenate([w, jnp.zeros((r, c - cols), f32)], axis=1)
    return w.T[:cols]


def column(row):
    count = row.shape[1]
    wide = up_to(count, LANES)
    if wide > count:
        row = jnp.concatenate([row, jnp.zeros((1, wide - count), f32)], axis=1)
    return jnp.broadcast_to(row, (LANES, wide)).T[:count]


def mixer_kernel(
    n_sp,
    n_tp,
    keep,
    x_hbm,
    wpool_hbm,
    wq_hbm,
    wkv_hbm,
    wkr_hbm,
    wqup_hbm,
    wkup_hbm,
    wvup_hbm,
    wop_hbm,
    woa_hbm,
    in_gain_hbm,
    pool_gain_hbm,
    qlat_gain_hbm,
    kvlat_gain_hbm,
    qh_gain_hbm,
    kh_gain_hbm,
    cos_q_hbm,
    sin_q_hbm,
    cos_k_hbm,
    sin_k_hbm,
    cos_b_hbm,
    sin_b_hbm,
    out_ref,
    in_gain,
    pool_gain,
    qlat_gain,
    kvlat_gain,
    qh_gain,
    kh_gain,
    cos_q,
    sin_q,
    cos_k,
    sin_k,
    cos_b,
    sin_b,
    x_own,
    wpool,
    wq_raw,
    wkv_raw,
    wkr_raw,
    wqup,
    wkup,
    wvup,
    wo,
    wo_p,
    wq_cat,
    wkv_cat,
    wq_t,
    wk_t,
    wv_pad,
    gain_q,
    gain_k,
    xg,
    qx,
    qy,
    kv_mine,
    kvx,
    rope_own,
    kv_all,
    pool_ext,
    queries,
    keys_t,
    values,
    acc,
    act,
    act_p,
    f_out,
    f_in,
    ld_sem,
    a_far_send,
    a_near_send,
    a_relay_send,
    a_recv,
    kv_send,
    kv_recv,
    q_far_send,
    q_near_send,
    q_relay_send,
    q_recv,
    up_send,
    side_send,
    near_send,
    x_send,
    d_recv,
    p_send,
    p_recv,
    wo_send,
    wo_recv,
    act_send,
    act_recv,
    f_send,
    f_recv,
):
    me = lax.axis_index("tp")
    core, chip = lax.rem(me, 2), lax.div(me, 2)
    chips = n_tp // 2
    partner = me + 1 - 2 * core
    shard = lax.axis_index("sp")
    deep, side = lax.div(shard, 2), lax.rem(shard, 2)
    last_deep = n_sp // 2 - 1
    other = shard + 1 - 2 * side

    r, width = x_own.shape
    rows = r * n_tp
    half = r * chips
    qc = wq_raw.shape[0]
    kc = wkv_raw.shape[1]
    kvlat = kc * n_tp
    pc = wpool.shape[1]
    heads = wkup.shape[1] // NOPE
    hc = heads * VDIM
    rc = r // CHUNKS

    packed = packs(qc, chips)

    def doubled(w):
        if not packed:
            return w
        rest = w[:, LANES:]
        return jnp.concatenate([w[:, :LANES], rest + pltpu.roll(rest, LANES // 2, 1)], axis=1)

    loads = {}

    def load(i, name, src, dst):
        loads[name] = pltpu.make_async_copy(src, dst, ld_sem.at[i])
        loads[name].start()

    load(0, "x", x_hbm, x_own)
    load(10, "in_gain", in_gain_hbm, in_gain)
    load(1, "wkv", wkv_hbm, wkv_raw)
    load(2, "wkr", wkr_hbm, wkr_raw)
    load(3, "wq", wq_hbm, wq_raw)
    load(4, "wpool", wpool_hbm, wpool)
    load(5, "wqup", wqup_hbm, wqup)
    load(6, "wkup", wkup_hbm, wkup)
    load(7, "wvup", wvup_hbm, wvup)
    load(8, "wop", wop_hbm, wo.at[pl.ds(0, pc), :])
    load(9, "woa", woa_hbm, wo.at[pl.ds(pc, hc), :])
    small = {
        "pool_gain": (pool_gain_hbm, pool_gain),
        "qlat_gain": (qlat_gain_hbm, qlat_gain),
        "kvlat_gain": (kvlat_gain_hbm, kvlat_gain),
        "qh_gain": (qh_gain_hbm, qh_gain),
        "kh_gain": (kh_gain_hbm, kh_gain),
        "cos_q": (cos_q_hbm, cos_q),
        "sin_q": (sin_q_hbm, sin_q),
        "cos_k": (cos_k_hbm, cos_k),
        "sin_k": (sin_k_hbm, sin_k),
        "cos_b": (cos_b_hbm, cos_b),
        "sin_b": (sin_b_hbm, sin_b),
    }
    for i, (name, pair) in enumerate(small.items()):
        load(11 + i, name, *pair)

    barrier = pltpu.get_barrier_semaphore()
    for step in range(1, n_tp):
        pl.semaphore_signal(
            barrier, inc=1, device_id={"tp": lax.rem(me + step, n_tp)}, device_id_type=MESH
        )
    greeted = n_tp - 1
    for gap in (-2, -1, 1, 2):
        there = shard + gap
        valid = (there >= 0) & (there < n_sp)

        @pl.when(valid)
        def _():
            pl.semaphore_signal(barrier, inc=1, device_id={"sp": there}, device_id_type=MESH)

        greeted = greeted + jnp.where(valid, 1, 0)
    pl.semaphore_wait(barrier, greeted)

    def place(k, c):
        return 2 * k + c

    def behind(step):
        return lax.rem(chip + chips - step, chips)

    def ahead(step):
        return lax.rem(chip + step, chips)

    def rows_at(g, off, count):
        return pl.ds(pl.multiple_of(g * r + off, 16), count)

    def arrived(ref, sem):
        remote(ref, ref, a_near_send.at[0], sem, {"tp": partner}).wait_recv()

    sends = []
    loads["x"].wait()
    loads["in_gain"].wait()
    for c in range(CHUNKS):
        at = pl.ds(c * rc, rc)
        xf = x_own[at, :].astype(f32)
        factor = lax.rsqrt(jnp.mean(xf * xf, axis=1, keepdims=True) + norm_eps)
        xg[me, at, :] = (xf * factor * in_gain[...]).astype(bf16)
        own = xg.at[me, at, :]
        for step in range(1, chips):
            copy = remote(
                own, own, a_far_send.at[step - 1, c], a_recv.at[me, c], {"tp": place(ahead(step), core)}
            )
            copy.start()
            sends.append(copy)
    for c in range(CHUNKS):
        own = xg.at[me, pl.ds(c * rc, rc), :]
        copy = remote(own, own, a_near_send.at[c], a_recv.at[me, c], {"tp": partner})
        copy.start()
        sends.append(copy)

    loads["wkv"].wait()
    loads["wkr"].wait()
    wkv_cat[:, :kc] = wkv_raw[...]
    wkv_cat[:, LANES:] = padded_transpose(wkr_raw[...]).astype(bf16)
    loads["wq"].wait()
    wq_cat[...] = doubled(padded_transpose(wq_raw[...])).astype(bf16)
    loads["wpool"].wait()

    def project_kv(k, c, off, count, same_core):
        both = dot(xg[place(k, c), pl.ds(off, count), :], wkv_cat[...])
        kv_mine[c, k, pl.ds(off, count), :] = both[:, :kc].astype(bf16)
        if same_core:
            shared = both[:, LANES : 2 * LANES].astype(bf16).astype(f32)
            rope_own[pl.ds(pl.multiple_of(k * r + off, 8), count), :] = shared

    def project_q(k, c, off, count):
        g = place(k, c)
        q = dot(xg[g, pl.ds(off, count), :], wq_cat[...]).astype(bf16)
        if packed:
            at = pl.ds(pl.multiple_of(k * r + off, 16), count)
            side_of = lax.broadcasted_iota(jnp.int32, (count, LANES), 1) // (LANES // 2)
            old, new = qy[me, at, :].astype(f32), q[:, LANES:].astype(f32)
            qy[me, at, :] = jnp.where(side_of == c, new, old).astype(bf16)
            q = q[:, :LANES]
        qx[me, rows_at(g, off, count), :] = q

    def project_pool(k, c, off, count):
        g = place(k, c)
        at_ext = pl.ds(pl.multiple_of(g * r + off + RIM, 16), count)
        pool_ext[at_ext, :] = dot(xg[g, pl.ds(off, count), :], wpool[...]).astype(bf16)

    def project(k, c, off, count, same_core):
        project_kv(k, c, off, count, same_core)
        project_q(k, c, off, count)
        project_pool(k, c, off, count)

    def kv_piece(source, k, off, count):
        return kvx.at[source, k, pl.ds(off, count), :]

    def send_kv(k, off, count, number):
        for step in range(1, n_tp):
            there = lax.rem(me + step, n_tp)
            copy = remote(
                kv_mine.at[lax.rem(there, 2), k, pl.ds(off, count), :],
                kv_piece(me, k, off, count),
                kv_send.at[step - 1, number],
                kv_recv.at[me, number],
                {"tp": there},
            )
            copy.start()
            sends.append(copy)

    project(chip, core, 0, r, True)
    for c in range(CHUNKS):
        arrived(xg.at[partner, pl.ds(c * rc, rc), :], a_recv.at[partner, c])
    project(chip, 1 - core, 0, r, False)
    send_kv(chip, 0, r, 0)

    loads["wqup"].wait()
    for name in small:
        loads[name].wait()
    lat_rows = qlat_gain[...]
    lat_gain = jnp.concatenate([column(lat_rows[i : i + 1]) for i in range(lat_rows.shape[0])], axis=0)
    gain_q[...] = column(qh_gain[...])
    gain_k[...] = column(kh_gain[...])
    for src in range(n_tp):
        span = slice(src * qc, (src + 1) * qc)
        part = wqup[span, :].astype(f32) * lat_gain[span, :1]
        wq_t[src] = doubled(padded_transpose(part)).astype(bf16)
    loads["wkup"].wait()
    wk_t[...] = padded_transpose(wkup[...]).astype(bf16)
    loads["wvup"].wait()
    wv_pad[...] = jnp.zeros_like(wv_pad)
    for h in range(heads):
        wv_pad[:, h * LANES : h * LANES + VDIM] = (
            wvup[...].astype(f32)[:, h * VDIM : (h + 1) * VDIM].astype(bf16)
        )
    acc[...] = jnp.zeros_like(acc)

    loads["wop"].wait()
    loads["woa"].wait()
    wo_copy = remote(wo, wo_p, wo_send, wo_recv, {"tp": partner})
    wo_copy.start()

    for c in range(CHUNKS):
        at = pl.ds(c * rc, rc)
        for step in range(1, chips):
            g = place(behind(step), core)
            block = xg.at[g, at, :]
            arrived(block, a_recv.at[g, c])
            copy = remote(block, block, a_relay_send.at[step - 1, c], a_recv.at[g, c], {"tp": partner})
            copy.start()
            sends.append(copy)
        for step in range(1, chips):
            project_kv(behind(step), core, c * rc, rc, True)
        if c < CHUNKS - 1:
            for step in range(1, chips):
                project_q(behind(step), core, c * rc, rc)
                project_pool(behind(step), core, c * rc, rc)
        for step in range(1, chips):
            g = place(behind(step), 1 - core)
            arrived(xg.at[g, at, :], a_recv.at[g, c])
            project_kv(behind(step), 1 - core, c * rc, rc, False)
            send_kv(behind(step), c * rc, rc, 1 + (step - 1) * CHUNKS + c)
            if c < CHUNKS - 1:
                project_q(behind(step), 1 - core, c * rc, rc)
                project_pool(behind(step), 1 - core, c * rc, rc)
    late = (CHUNKS - 1) * rc
    for step in range(1, chips):
        project_q(behind(step), core, late, rc)
        project_q(behind(step), 1 - core, late, rc)

    q_parts = (qx, qy) if packed else (qx,)
    for i, whole in enumerate(q_parts):
        own_q = whole.at[me]
        for step in range(1, chips):
            copy = remote(
                own_q, own_q, q_far_send.at[step - 1, i], q_recv.at[me, i], {"tp": place(ahead(step), core)}
            )
            copy.start()
            sends.append(copy)
    for i, whole in enumerate(q_parts):
        own_q = whole.at[me]
        copy = remote(own_q, own_q, q_near_send.at[i], q_recv.at[me, i], {"tp": partner})
        copy.start()
        sends.append(copy)

    for step in range(1, chips):
        project_pool(behind(step), core, late, rc)
        project_pool(behind(step), 1 - core, late, rc)

    rim_copy = remote(
        pool_ext.at[pl.ds(rows, RIM), :], pool_ext.at[pl.ds(0, RIM), :], p_send, p_recv, {"sp": shard + 1}
    )

    @pl.when(shard < n_sp - 1)
    def _():
        rim_copy.start()

    @pl.when(shard == 0)
    def _():
        pool_ext[pl.ds(0, RIM), :] = jnp.zeros((RIM, pc), bf16)

    kvx[me] = kv_mine[core]
    for step in range(1, n_tp):
        source = lax.rem(me + step, n_tp)
        its_chip = lax.div(source, 2)
        arrived(kv_piece(source, its_chip, 0, r), kv_recv.at[source, 0])
        for hop in range(1, chips):
            k = lax.rem(its_chip + chips - hop, chips)
            for c in range(CHUNKS):
                number = 1 + (hop - 1) * CHUNKS + c
                arrived(kv_piece(source, k, c * rc, rc), kv_recv.at[source, number])
    p = crossed(r)

    def permuted(x):
        width = x.shape[2]
        return jnp.concatenate(
            [x[:, :p].reshape(chips * p, width), x[:, p:].reshape(chips * (r - p), width)], axis=0
        )

    lat = jnp.concatenate([permuted(kvx[i].astype(f32)) for i in range(n_tp)], axis=1)
    factor = lax.rsqrt(jnp.mean(lat * lat, axis=1, keepdims=True) + norm_eps)
    kv_all[shard, core, pl.ds(0, half), :] = (lat * factor * kvlat_gain[...]).astype(bf16)
    kv_all[shard, core, pl.ds(half, ROPE), pl.ds(0, half)] = permuted(rope_own[...].reshape(chips, r, LANES)).T[:ROPE].astype(bf16)

    tail = chips * p

    def head_rows(block, h, k):
        return kv_all.at[block, h, pl.ds(pl.multiple_of(k * p, 16), p), :]

    def tail_rows(block, h):
        return kv_all.at[block, h, pl.ds(tail, half - tail + ROPE), :]

    def parts_of(block):
        return (head_rows(block, core, chip), tail_rows(block, core))

    def to_shard(block, i, send, there):
        ref = parts_of(block)[i]
        sem = d_recv.at[block, core, chip if i == 0 else chips]
        return remote(ref, ref, send.at[block, i], sem, {"sp": there})

    def onward(block, i):
        return to_shard(block, i, up_send, shard + 2)

    def across(block, i):
        return to_shard(block, i, side_send, other)

    def over(block, step):
        ref = head_rows(block, core, chip)
        return remote(
            ref, ref, x_send.at[block, step - 1], d_recv.at[block, core, chip], {"tp": place(ahead(step), core)}
        )

    def near(block, k):
        ref = head_rows(block, core, k)
        return remote(ref, ref, near_send.at[block, k], d_recv.at[block, core, k], {"tp": partner})

    def near_tail(block):
        ref = tail_rows(block, core)
        return remote(ref, ref, near_send.at[block, chips], d_recv.at[block, core, chips], {"tp": partner})

    for i in range(2):

        @pl.when(deep < last_deep)
        def _():
            onward(shard, i).start()

        @pl.when(side == 0)
        def _():
            across(shard, i).start()

    for k in range(chips):
        near(shard, k).start()
    near_tail(shard).start()

    score_scale = HEAD ** (-0.5) * math.log2(math.e)
    q_tile = 2 * r

    def table(cos_ref, sin_ref, block, at):
        ca, sa = cos_ref[:, at], sin_ref[:, at]
        cb, sb = cos_b[block], sin_b[block]
        return ca * cb - sa * sb, sa * cb + ca * sb

    def make_queries(i, _):
        at = pl.ds(pl.multiple_of(i * half, half), half)
        raw = None
        squares = None
        ones = jnp.ones((8, wq_t.shape[2]), bf16)
        for src in range(n_tp):
            part = qx[src, at, :]
            if packed:
                rest = qy[src, pl.ds(pl.multiple_of(i * r, r), r), :].astype(f32)
                side_of = lax.broadcasted_iota(jnp.int32, rest.shape, 1) // (LANES // 2)
                rest = [jnp.where(side_of == c, rest, 0.0).astype(bf16) for c in range(2)]
                part = jnp.concatenate([part, jnp.concatenate(rest, axis=0)], axis=1)
            term = dot_nt(wq_t[src], part)
            raw = term if raw is None else raw + term
            pf = part.astype(f32)
            term = dot_nt(ones, (pf * pf).astype(bf16))
            squares = term if squares is None else squares + term
        eps = norm_eps * (squares[:1] * (1.0 / (qc * n_tp)) + norm_eps)
        cosine, sine = table(cos_q, sin_q, shard, at)
        for h in range(heads):
            x = raw[h * HEAD : (h + 1) * HEAD]
            factor = lax.rsqrt(jnp.sum(x * x, axis=0, keepdims=True) * (1.0 / HEAD) + eps) * score_scale
            y = x * factor * gain_q[:, :1]
            low, high = y[NOPE : NOPE + HALF], y[NOPE + HALF :]
            full = jnp.concatenate(
                [
                    y[:NOPE] * gain_k[:NOPE, :1],
                    low * cosine - high * sine,
                    high * cosine + low * sine,
                    jnp.zeros((LANES - HEAD, half), f32),
                ],
                axis=0,
            )
            queries[h, at, :] = full.T.astype(bf16)
        return 0


    lane = lax.broadcasted_iota(jnp.int32, (half, LANES), 1)

    def prepare(block):
        slot = block if keep else 0
        for c in range(2):
            at = pl.ds(c * half, half)
            lat = kv_all[block, c, pl.ds(0, half), :]
            shared = kv_all[block, c, pl.ds(half, ROPE), pl.ds(0, half)].astype(f32)
            shared_sq = jnp.sum(shared * shared, axis=0, keepdims=True)
            cosine, sine = table(cos_k, sin_k, block, at)
            gained = shared * gain_k[NOPE:, :1]
            low, high = gained[:HALF], gained[HALF:]
            turned = jnp.concatenate([low * cosine - high * sine, high * cosine + low * sine], axis=0)
            plain = dot_nt(wk_t[...], lat)
            value = dot(lat, wv_pad[...])
            for h in range(heads):
                x = plain[h * NOPE : (h + 1) * NOPE]
                total = jnp.sum(x * x, axis=0, keepdims=True) + shared_sq
                factor = lax.rsqrt(total * (1.0 / HEAD) + norm_eps)
                keys_t[slot, h, :NOPE, at] = (x * factor).astype(bf16)
                keys_t[slot, h, NOPE:HEAD, at] = (turned * factor).astype(bf16)
                keys_t[slot, h, HEAD:, at] = jnp.zeros((LANES - HEAD, half), bf16)
                v = jnp.where(lane == VDIM, 1.0, value[:, h * LANES : (h + 1) * LANES])
                values[slot, h, at, :] = v.astype(bf16)

    key_tile = math.gcd(rows, 256)
    runs = key_runs(n_tp, r)

    def accumulate(block, i, masked):
        attend(block, i * q_tile, q_tile, masked)

    def attend(block, row, count, masked):
        slot = block if keep else 0
        at = pl.ds(pl.multiple_of(row, r), count)
        for h in range(heads):
            q = queries[h, at, :]
            total = acc[h, at, :]
            for j in range(rows // key_tile):
                cols = pl.ds(j * key_tile, key_tile)
                weights = jnp.exp2(dot(q, keys_t[slot, h, :, cols]))
                if masked:
                    q_pos = row + lax.broadcasted_iota(jnp.int32, weights.shape, 0)
                    col = j * key_tile + lax.broadcasted_iota(jnp.int32, weights.shape, 1)
                    k_pos = col
                    shift = 0
                    for start, first in runs:
                        if first - start != shift and start < (j + 1) * key_tile:
                            k_pos = k_pos + jnp.where(col >= start, first - start - shift, 0)
                            shift = first - start
                    weights = jnp.where(k_pos <= q_pos, weights, 0.0)
                total = total + dot(weights.astype(bf16), values[slot, h, cols, :])
            acc[h, at, :] = total

    def far_rows(block, masked):
        def one(step, _):
            accumulate(block, lax.rem(chip + step, chips), masked)
            return 0

        lax.fori_loop(1, chips, one, 0)

    def early_rows(block, masked):
        far_rows(block, masked)
        if not keep:
            accumulate(block, chip, masked)

    def z_block(e):
        return shard - 2 * e

    def y_block(e):
        return other - 2 * (e - 1)

    def y_valid(e):
        return (e - 1 >= 1 - side) & (e - 1 <= deep)

    def pass_on(block, from_z):
        for i in range(2):
            arrived(parts_of(block)[i], d_recv.at[block, core, chip if i == 0 else chips])
            if from_z:

                @pl.when(deep < last_deep)
                def _():
                    onward(block, i).start()

                across(block, i).start()
            if i == 0:
                for step in range(1, chips):
                    over(block, step).start()
                near(block, chip).start()
            else:
                near_tail(block).start()

    def forward(e):
        @pl.when(e <= deep)
        def _():
            pass_on(z_block(e), True)

        @pl.when(y_valid(e))
        def _():
            pass_on(y_block(e), False)

    def relay(block):
        for step in range(1, chips):
            k = behind(step)
            arrived(head_rows(block, core, k), d_recv.at[block, core, k])
            near(block, k).start()

    def ready(block):
        for k in range(chips):
            arrived(head_rows(block, 1 - core, k), d_recv.at[block, 1 - core, k])
        arrived(tail_rows(block, 1 - core), d_recv.at[block, 1 - core, chips])
        prepare(block)

    @pl.when(shard > 0)
    def _():
        arrived(pool_ext.at[pl.ds(0, RIM), :], p_recv)

    def pool(i, _):
        base = pl.multiple_of(i * LANES, LANES)
        ext = pool_ext[pl.ds(base, LANES + RIM), :].astype(f32)
        channel = me * pc + lax.broadcasted_iota(jnp.int32, (LANES, pc), 1)
        window = jnp.left_shift(jnp.int32(2), lax.div(channel, GROUP))
        total = ext
        chosen = None
        for level in range(4):
            total = total + pltpu.roll(total, 1 << level, 0)
            if chosen is None:
                chosen = total[RIM:]
            else:
                chosen = jnp.where(window >= (2 << level), total[RIM:], chosen)
        position = shard * rows + base + lax.broadcasted_iota(jnp.int32, (LANES, pc), 0)
        divisor = jnp.minimum(position + 1, window).astype(f32)
        pooled = (chosen / divisor - ext[RIM:]) * pool_gain[...]
        act[pl.ds(base, LANES), :pc] = pooled.astype(bf16)
        return 0

    lax.fori_loop(0, rows // LANES, pool, 0)

    forward(1)

    for i, whole in enumerate(q_parts):
        for step in range(1, chips):
            block = whole.at[place(behind(step), core)]
            sem = q_recv.at[place(behind(step), core), i]
            arrived(block, sem)
            copy = remote(block, block, q_relay_send.at[step - 1, i], sem, {"tp": partner})
            copy.start()
            sends.append(copy)
    for i, whole in enumerate(q_parts):
        for k in range(chips):
            g = place(k, 1 - core)
            arrived(whole.at[g], q_recv.at[g, i])

    lax.fori_loop(0, 2, make_queries, 0)

    ready(shard)
    early_rows(shard, True)

    def reach(e):
        return 2 * (e - 1)

    def one_event(e, _):
        forward(e)

        def pick(i):
            k = lax.div(i + 1, 2)
            first = lax.rem(i, 2) == 1
            return jnp.where(first, z_block(k), y_block(k)), first | y_valid(k)

        def relay_at(i):
            block, valid = pick(i)

            @pl.when(valid & (i <= reach(e)))
            def _():
                relay(block)

        def one(i, _):
            relay_at(i + 1)
            block, valid = pick(i)

            @pl.when(valid)
            def _():
                ready(block)
                early_rows(block, False)

            return 0

        relay_at(reach(e - 1) + 1)
        lax.fori_loop(reach(e - 1) + 1, reach(e) + 1, one, 0)
        return 0

    lax.fori_loop(2, deep + 2, one_event, 0)
    final = y_block(deep + 1)
    has_final = y_valid(deep + 1)

    @pl.when(has_final)
    def _():
        relay(final)
        ready(final)

    def finish(k, c):
        at = rows_at(place(k, c), 0, r)
        parts = []
        for h in range(heads):
            a = acc[h, at, :]
            parts.append(a[:, :VDIM] / a[:, VDIM : VDIM + 1])
        act[at, pc:] = jnp.concatenate(parts, axis=1).astype(bf16)

    def hand_over(k):
        finish(k, 1 - core)
        copy = remote(
            act.at[rows_at(place(k, 1 - core), 0, r), :], act_p.at[k], act_send.at[k], act_recv.at[k], {"tp": partner}
        )
        copy.start()
        sends.append(copy)

    def last_block(k, c):
        @pl.when(has_final)
        def _():
            attend(final, place(k, c) * r, r, False)

    cw = width // COLS

    def product(k, n):
        cols = pl.ds(n * cw, cw)
        mine = act[rows_at(place(k, core), 0, r), :]
        return dot(mine, wo[:, cols]) + dot(act_p[k], wo_p[:, cols])

    for step in range(1, chips):
        last_block(ahead(step), 1 - core)
        hand_over(ahead(step))
    for step in range(1, chips):
        last_block(ahead(step), core)
        finish(ahead(step), core)
    arrived(wo_p, wo_recv)
    for step in range(1, chips):
        k = ahead(step)
        arrived(act_p.at[k], act_recv.at[k])
        for n in range(COLS):
            f_out[step - 1, n] = product(k, n).astype(bf16)
            copy = remote(
                f_out.at[step - 1, n],
                f_in.at[step - 1, n],
                f_send.at[step - 1, n],
                f_recv.at[step - 1, n],
                {"tp": place(k, core)},
            )
            copy.start()
            sends.append(copy)

    if keep:
        accumulate(shard, chip, True)

        def own_rows(block, _):
            accumulate(block, chip, False)
            return 0

        lax.fori_loop(0, shard, own_rows, 0)
    else:

        @pl.when(has_final)
        def _():
            accumulate(final, chip, False)

    hand_over(chip)
    finish(chip, core)
    arrived(act_p.at[chip], act_recv.at[chip])
    for n in range(COLS):
        total = product(chip, n)
        for step in range(1, chips):
            arrived(f_in.at[step - 1, n], f_recv.at[step - 1, n])
            total = total + f_in[step - 1, n].astype(f32)
        out_ref[:, n * cw : (n + 1) * cw] = total.astype(bf16)

    for copy in sends:
        copy.wait_send()
    wo_copy.wait_send()

    @pl.when(shard < n_sp - 1)
    def _():
        rim_copy.wait_send()

    def drain(j, _):
        block = shard - j
        column = lax.rem(j, 2) == 0
        for k in range(chips):
            near(block, k).wait_send()
        near_tail(block).wait_send()

        @pl.when(j > 0)
        def _():
            for step in range(1, chips):
                over(block, step).wait_send()

        for i in range(2):

            @pl.when(column & (deep < last_deep))
            def _():
                onward(block, i).wait_send()

            @pl.when(column & ((j > 0) | (side == 0)))
            def _():
                across(block, i).wait_send()

        return 0

    lax.fori_loop(0, shard + 1, drain, 0)


def vmem_bytes(arrays):
    total = 0
    for shape, kind in arrays:
        size = 2 if kind == bf16 else 4
        minor = up_to(shape[-1], LANES) * up_to(shape[-2], 32 // size) * size
        total += math.prod(shape[:-2]) * minor
    return total


def packs(qc, chips):
    return chips == 2 and qc == LANES + LANES // 2


def crossed(r):
    return r * 5 // 6


def key_runs(n_tp, r):
    chips, p = n_tp // 2, crossed(r)
    runs = []
    for c in range(2):
        base = c * chips * r
        runs += [(base + k * p, (2 * k + c) * r) for k in range(chips)]
        runs += [(base + chips * p + k * (r - p), (2 * k + c) * r + p) for k in range(chips)]
    return runs


def tables(n_sp, n_tp, rows):
    frequency = np.float32(rope_theta) ** (-np.arange(0, ROPE, 2, dtype=np.float32) / np.float32(ROPE))
    r = rows // n_tp

    def make(positions):
        angles = frequency.astype(np.float32)[:, None] * positions.astype(np.float32)[None, :]
        angles = angles.astype(np.float64)
        return np.cos(angles).astype(np.float32), np.sin(angles).astype(np.float32)

    natural = np.arange(rows)
    runs = key_runs(n_tp, r) + [(rows, 0)]
    split = np.concatenate([first + np.arange(runs[i + 1][0] - at) for i, (at, first) in enumerate(runs[:-1])])
    blocks = make(np.arange(n_sp) * rows)
    columns = [np.ascontiguousarray(t.T)[:, :, None] for t in blocks]
    return [*make(natural), *make(split), *columns]


def local(
    activations,
    in_gain,
    w_pool_in,
    pool_gain,
    w_qlat,
    w_kvlat,
    w_krope,
    qlat_gain,
    kvlat_gain,
    w_qup,
    w_kup,
    w_vup,
    qhead_gain,
    khead_gain,
    w_out_pool,
    w_out_attn,
):
    n_sp, n_tp = lax.axis_size("sp"), lax.axis_size("tp")
    r, width = activations.shape
    rows, chips = r * n_tp, n_tp // 2
    half = r * chips
    others = max(1, chips - 1)
    w_qlat, w_krope = w_qlat.T, w_krope.T
    qc, kc, pc = w_qlat.shape[0], w_kvlat.shape[1], w_pool_in.shape[1]
    heads = w_kup.shape[1] // NOPE
    kvlat = w_kup.shape[0]
    hc = heads * VDIM
    qp = up_to(qc, LANES)
    vm = pl.BlockSpec(memory_space=pltpu.VMEM)
    hbm = pl.BlockSpec(memory_space=pltpu.MemorySpace.HBM)
    small = [
        in_gain.reshape(1, -1),
        pool_gain.reshape(1, -1),
        qlat_gain.reshape(-1, LANES),
        kvlat_gain.reshape(1, -1),
        qhead_gain.reshape(1, -1),
        khead_gain.reshape(1, -1),
    ] + [jnp.asarray(t) for t in tables(n_sp, n_tp, rows)]
    def scratch_of(slots):
      return [(t.shape, f32) for t in small] + [
        ((r, width), bf16),
        ((width, pc), bf16),
        ((qc, width), bf16),
        ((width, kc), bf16),
        (w_krope.shape, bf16),
        (w_qup.shape, bf16),
        (w_kup.shape, bf16),
        (w_vup.shape, bf16),
        ((pc + hc, width), bf16),
        ((pc + hc, width), bf16),
        ((width, qp), bf16),
        ((width, 2 * LANES), bf16),
        ((n_tp, heads * HEAD, qp), bf16),
        ((heads * NOPE, kvlat), bf16),
        ((kvlat, heads * LANES), bf16),
        ((HEAD, LANES), f32),
        ((HEAD, LANES), f32),
        ((n_tp, r, width), bf16),
        ((n_tp, rows, LANES if packs(qc, chips) else qp), bf16),
        ((n_tp, half, LANES), bf16),
        ((2, chips, r, kc), bf16),
        ((n_tp, chips, r, kc), bf16),
        ((half, LANES), f32),
        ((n_sp, 2, half + ROPE, kvlat), bf16),
        ((rows + RIM, pc), bf16),
        ((heads, rows, LANES), bf16),
        ((slots, heads, LANES, rows), bf16),
        ((slots, heads, rows, LANES), bf16),
        ((heads, rows, LANES), f32),
        ((rows, pc + hc), bf16),
        ((chips, r, pc + hc), bf16),
        ((others, COLS, r, width // COLS), bf16),
        ((others, COLS, r, width // COLS), bf16),
    ]
    keep = vmem_bytes(scratch_of(n_sp)) + SPARE <= VMEM_MOST
    scratch = scratch_of(n_sp if keep else 1)
    dma = pltpu.SemaphoreType.DMA
    sems = [
        (22,),
        (others, CHUNKS),
        (CHUNKS,),
        (others, CHUNKS),
        (n_tp, CHUNKS),
        (n_tp, 1 + others * CHUNKS),
        (n_tp, 1 + others * CHUNKS),
        (others, 2),
        (2,),
        (others, 2),
        (n_tp, 2),
        (n_sp, 2),
        (n_sp, 2),
        (n_sp, chips + 1),
        (n_sp, others),
        (n_sp, 2, chips + 1),
        None,
        None,
        None,
        None,
        (chips,),
        (chips,),
        (others, COLS),
        (others, COLS),
    ]
    return pl.pallas_call(
        functools.partial(mixer_kernel, n_sp, n_tp, keep),
        out_shape=jax.ShapeDtypeStruct((r, width), bf16),
        in_specs=[hbm] * (10 + len(small)),
        out_specs=vm,
        scratch_shapes=[pltpu.VMEM(s, d) for s, d in scratch] + [dma if s is None else dma(s) for s in sems],
        compiler_params=pltpu.CompilerParams(
            collective_id=0, has_side_effects=True, vmem_limit_bytes=min(VMEM_MOST, vmem_bytes(scratch) + SPARE)
        ),
    )(*[pltpu.with_memory_space_constraint(t, pltpu.MemorySpace.HBM) for t in (
        activations,
        w_pool_in,
        w_qlat,
        w_kvlat,
        w_krope,
        w_qup,
        w_kup,
        w_vup,
        w_out_pool,
        w_out_attn,
        *small)]
    )


def solution(mesh):
    placed = (
        P(("sp", "tp"), None),
        P(),
        P(None, "tp"),
        P("tp"),
        P(None, "tp"),
        P(None, "tp"),
        P(),
        P(),
        P(),
        P(None, "tp"),
        P(None, "tp"),
        P(None, "tp"),
        P(),
        P(),
        P("tp", None),
        P("tp", None),
    )
    return jax.shard_map(
        local, mesh=mesh, in_specs=placed, out_specs=P(("sp", "tp"), None), check_vma=False
    )
```
